32 devices in a mesh: grp: 2 (over y), sp: 4 (over z), tp: 4 (over x, core).
Axes of the slice: x: 2, y: 2, z: 4, core: 2. Of those that a mesh axis runs over, the one named last changes fastest.
Arguments:
- latent: bfloat16 [3072, 2048], P(('grp', 'sp')), parts along dimension 0, may hold values from -6 to 6
- conditioning: bfloat16 [4096], P(('grp', 'sp')), parts along dimension 0, may hold values from -6 to 6
- context: bfloat16 [128, 2048], P(('grp', 'sp')), parts along dimension 0, may hold values from -6 to 6
- ctx_vector: bfloat16 [2048], P('sp'), may hold values from -6 to 6
- w_shift: bfloat16 [2048, 2048], P('sp', 'tp'), may hold values from -0.25 to 0.25
- w_scale: bfloat16 [2048, 2048], P('sp', 'tp'), may hold values from -0.25 to 0.25
- w_gate: bfloat16 [2048, 2048], P('sp', 'tp'), may hold values from -0.25 to 0.25
- norm_gain: bfloat16 [2048], replicated, may hold values from 0.099609375 to 1.8984375
- w_query: bfloat16 [2048, 1024], P(None, 'tp'), may hold values from -1 to 1
- w_key: bfloat16 [2048, 1024], P(None, 'tp'), may hold values from -1 to 1
- w_value: bfloat16 [2048, 1024], P(None, 'tp'), may hold values from -0.125 to 0.125
- offset_bias: float32 [16, 15, 31], P('tp'), may hold values from 1.5 to 4.5
- w_out: bfloat16 [1024, 2048], P(None, 'tp'), may hold values from -0.75 to 0.75
Outputs:
- mixed_out: bfloat16 [3072, 2048], P(('grp', 'sp'), 'tp'), parts along dimension 0
The draws below stay inside these ranges and needn't reach their ends.
There are 2 independent parts, one for each index of `grp`. The reference program is written for one: setup_inputs(seed, part) draws one part's arguments, and reference() takes and returns one part's arrays. A program takes and returns all parts, laid end to end along the dimension named above; an argument that names none is the same for every part. Nothing has to cross between parts.
All inputs are finite; a program needn't handle non-finite values.
Results may differ from the reference program's by a relative error of at most 0.011.
Values may be sent and summed in bfloat16 or wider, within the bound.
No kernel may reach another device: no remote copies, remote signals or barrier semaphores. Data moves between devices by JAX's collectives and lax.ppermute only.
A program may use at most 64 MiB of HBM per device.

```python
import jax
import jax.numpy as jnp
from jax import lax

D = 2048
HEADS = 16
HEAD_DIM = 64
GRID_W = 64
WIN_H = 8
WIN_W = 16
ROWS_DEV = 6
TOKENS = 1536
CTX = 64
WIDTH = 1024
N_SP = 4


def weight_pair(key):
    base_key = jax.random.fold_in(key, 101)
    first_key, second_key = jax.random.split(base_key, 2)
    columns = HEADS * HEAD_DIM
    first = jax.random.normal(first_key, (D, columns), jnp.float32) * D ** (-0.5)
    second = jax.random.normal(second_key, (D, columns), jnp.float32) * D ** (-0.5)
    query_weight = first
    key_weight = second
    return (jnp.clip(query_weight, -1.0, 1.0), jnp.clip(key_weight, -1.0, 1.0))


def draw_w_query(key, part):
    return weight_pair(key)[0].astype(jnp.bfloat16)


def draw_w_key(key, part):
    return weight_pair(key)[1].astype(jnp.bfloat16)


def level_of(key, extent, cuts, smallest, top_value):
    gain, own = 1.0, jax.random.fold_in(key, 6)
    for dim, parts in cuts:
        heights = jnp.exp(jax.random.uniform(jax.random.fold_in(own, dim), (parts,), jnp.float32, smallest / len(cuts), top_value / len(cuts)))
        gain = gain * jnp.repeat(heights, extent[dim] // parts).reshape([-1 if axis == dim else 1 for axis in range(len(extent))])
    return gain


def noise(rng, extent, spread, reach, cuts=(), held_as=jnp.bfloat16):
    loudness = level_of(rng, extent, cuts, -0.22, 0.18) if cuts else 1.0
    values = jax.random.normal(rng, extent, jnp.float32) * spread * loudness
    return jnp.minimum(jnp.maximum(values, -reach), reach).astype(held_as)


def setup_inputs(seed: int = 0, part: int = 0) -> dict:
    streams_of = jax.random.split(jax.random.key(seed), 14)
    part_splits = jax.random.split(jax.random.fold_in(streams_of[13], part), 14)
    latent = noise(part_splits[0], (TOKENS, D), 1.0, 6.0, ((0, 4),))
    conditioning = noise(part_splits[1], (D,), 1.0, 6.0, ((0, 4),))
    context = noise(part_splits[2], (CTX, D), 1.0, 6.0, ((0, 4),))
    ctx_vector = noise(streams_of[3], (D,), 1.0, 6.0, ((0, 4),))
    w_shift = noise(streams_of[4], (D, D), (D // 4) ** -0.5, 0.25, ((0, 4), (1, 4)))
    w_scale = noise(streams_of[5], (D, D), (D // 4) ** -0.5, 0.25, ((0, 4), (1, 4)))
    w_gate = noise(streams_of[6], (D, D), (D // 4) ** -0.5, 0.25, ((0, 4), (1, 4)))
    norm_gain = jnp.clip(1.0 + 0.18 * jax.random.normal(streams_of[7], (D,), jnp.float32), 0.099609375, 1.8984375).astype(jnp.bfloat16)
    w_query = draw_w_query(jax.random.fold_in(streams_of[13], 71), part)
    w_key = draw_w_key(jax.random.fold_in(streams_of[13], 71), part)
    w_value = noise(streams_of[10], (D, WIDTH), D ** -0.5, 0.125, ((1, 4),))
    offset_bias = jnp.clip(1.5 + 3.0 * jax.random.uniform(streams_of[11], (HEADS, 2 * WIN_H - 1, 2 * WIN_W - 1), jnp.float32) ** level_of(streams_of[11], (HEADS, 2 * WIN_H - 1, 2 * WIN_W - 1), ((0, 4),), -0.2, 0.2), 1.5, 4.5)
    w_out = noise(streams_of[12], (WIDTH, D), (WIDTH // 16) ** -0.5, 0.75, ((1, 4),))
    return dict(latent=latent, conditioning=conditioning, context=context, ctx_vector=ctx_vector, w_shift=w_shift, w_scale=w_scale, w_gate=w_gate, norm_gain=norm_gain, w_query=w_query, w_key=w_key, w_value=w_value, offset_bias=offset_bias, w_out=w_out)


EPSILON = 1e-06

def modulated_norm(inputs, norm_gain, shift_vec, scale_vec):
    floats = inputs.astype(jnp.float32)
    inverse = lax.rsqrt(lax.optimization_barrier(jnp.mean(floats * floats, axis=-1, keepdims=True)) + EPSILON)
    return (floats * inverse * norm_gain.astype(jnp.float32) * (1.0 + scale_vec) + shift_vec).astype(jnp.bfloat16)

def project(inputs, weight):
    return jnp.dot(inputs, weight, preferred_element_type=jnp.float32).astype(jnp.bfloat16)

def reference(latent, conditioning, context, ctx_vector, w_shift, w_scale, w_gate, norm_gain, w_query, w_key, w_value, offset_bias, w_out):
    cond_act = jax.nn.silu(conditioning.astype(jnp.float32)).astype(jnp.bfloat16)
    ctx_act = jax.nn.silu(ctx_vector.astype(jnp.float32)).astype(jnp.bfloat16)
    shift_vec = jnp.dot(cond_act, w_shift, preferred_element_type=jnp.float32)
    scale_vec = jnp.dot(cond_act, w_scale, preferred_element_type=jnp.float32)
    gate_vec = jnp.dot(cond_act, w_gate, preferred_element_type=jnp.float32)
    ctx_shift = jnp.dot(ctx_act, w_shift, preferred_element_type=jnp.float32)
    ctx_scale = jnp.dot(ctx_act, w_scale, preferred_element_type=jnp.float32)
    normed = modulated_norm(latent, norm_gain, shift_vec, scale_vec)
    ctx_normed = modulated_norm(context, norm_gain, ctx_shift, ctx_scale)
    queries = project(normed, w_query)
    keys_lat = project(normed, w_key)
    values_lat = project(normed, w_value)
    ctx_keys = project(ctx_normed, w_key).astype(jnp.float32).reshape(-1, HEADS, HEAD_DIM)
    ctx_values = project(ctx_normed, w_value).astype(jnp.float32).reshape(-1, HEADS, HEAD_DIM)
    grid_rows = ROWS_DEV * N_SP
    query_grid = queries.astype(jnp.float32).reshape(grid_rows, GRID_W, HEADS, HEAD_DIM)
    key_grid = keys_lat.astype(jnp.float32).reshape(grid_rows, GRID_W, HEADS, HEAD_DIM)
    value_grid = values_lat.astype(jnp.float32).reshape(grid_rows, GRID_W, HEADS, HEAD_DIM)
    columns = jnp.arange(GRID_W, dtype=jnp.int32)
    col_index = jnp.clip(columns - WIN_W // 2, 0, GRID_W - WIN_W)[:, None] + jnp.arange(WIN_W, dtype=jnp.int32)[None, :]
    col_offset = (col_index - columns[:, None] + WIN_W - 1).astype(jnp.int32)
    scale_qk = HEAD_DIM ** (-0.5)
    bias_table = offset_bias.astype(jnp.float32)

    def one_row(grid_row):
        first_row = jnp.clip(grid_row - WIN_H // 2, 0, grid_rows - WIN_H).astype(jnp.int32)
        key_rows = lax.dynamic_slice_in_dim(key_grid, first_row, WIN_H, 0)
        value_rows = lax.dynamic_slice_in_dim(value_grid, first_row, WIN_H, 0)
        key_window = key_rows[:, col_index]
        value_window = value_rows[:, col_index]
        query_row = lax.dynamic_index_in_dim(query_grid, grid_row, 0, keepdims=False)
        row_offset = (first_row + jnp.arange(WIN_H, dtype=jnp.int32) - grid_row + WIN_H - 1).astype(jnp.int32)
        offset_terms = bias_table[:, row_offset[:, None, None], col_offset[None, :, :]]
        win_scores = jnp.einsum('chd,icjhd->hcij', query_row, key_window) * scale_qk + offset_terms.transpose(0, 2, 1, 3)
        ctx_scores = jnp.einsum('chd,lhd->hcl', query_row, ctx_keys) * scale_qk
        logits = jnp.concatenate([win_scores.reshape(HEADS, GRID_W, WIN_H * WIN_W), ctx_scores], axis=-1)
        rounded = jax.nn.softmax(logits, axis=-1).astype(jnp.bfloat16)
        weights = lax.optimization_barrier(rounded).astype(jnp.float32)
        win_weights = weights[..., :WIN_H * WIN_W].reshape(HEADS, GRID_W, WIN_H, WIN_W)
        result = jnp.einsum('hcij,icjhd->chd', win_weights, value_window)
        result = result + jnp.einsum('hcl,lhd->chd', weights[..., WIN_H * WIN_W:], ctx_values)
        return result.astype(jnp.bfloat16)
    attended = lax.map(one_row, jnp.arange(grid_rows, dtype=jnp.int32))
    attended = attended.reshape(grid_rows * GRID_W, HEADS * HEAD_DIM)
    branch = jnp.dot(attended, w_out, preferred_element_type=jnp.float32)
    return (latent.astype(jnp.float32) + gate_vec * branch).astype(jnp.bfloat16)
```

```python
import functools

import jax
import jax.numpy as jnp
from jax import lax
from jax.experimental import pallas as pl
from jax.experimental.pallas import tpu as pltpu
from jax.sharding import PartitionSpec as P

HEAD_DIM = 64
GRID_W = 64
WIN_H = 8
WIN_W = 16
EPSILON = 1e-06
HALO = WIN_H // 2
MASKED = -1e30
SHIFT, CTX_SHIFT, SCALE, CTX_SCALE, GATE, MOD_ROWS = 0, 1, 2, 3, 4, 8

F32 = jnp.float32
BF16 = jnp.bfloat16


def call(kernel, out_shape, scratch=(), vmem_mib=24, **kwargs):
    return pl.pallas_call(
        kernel,
        out_shape=out_shape,
        scratch_shapes=list(scratch),
        compiler_params=pltpu.CompilerParams(vmem_limit_bytes=vmem_mib * 2**20),
        **kwargs,
    )


def shape_of(shape, dtype):
    return jax.ShapeDtypeStruct(shape, dtype)


def digits(count):
    unit, found = 1, []
    while unit < count:
        radix = 4 if count // unit % 4 == 0 else 2
        found.append((unit, radix))
        unit *= radix
    return found


def peer(block, axis, mask):
    count = lax.axis_size(axis)
    return lax.ppermute(block, axis, [(i, i ^ mask) for i in range(count)])


def total(block, axis):
    for unit, radix in digits(lax.axis_size(axis)):
        parts = [peer(block, axis, unit * k) for k in range(1, radix)]
        for part in parts:
            block = block + part
    return block


def pieces_of(block, axis):
    pieces = [block]
    for unit, radix in digits(lax.axis_size(axis)):
        pieces = pieces + [peer(p, axis, unit * k) for k in range(1, radix) for p in pieces]
    return pieces


def pieces_by_bits(block, axis):
    pieces = [(0, block)]
    bit = lax.axis_size(axis) // 2
    while bit:
        pieces = pieces + [(mask ^ bit, peer(p, axis, bit)) for mask, p in pieces]
        bit //= 2
    return pieces


def pairwise(block, axis, first):
    count = lax.axis_size(axis)
    pairs = []
    for low in range(first, count - 1, 2):
        pairs += [(low, low + 1), (low + 1, low)]
    return lax.ppermute(block, axis, pairs)


def silu(v):
    return v / (1.0 + jnp.exp(-v))


def modulation_kernel(cond_ref, ctx_ref, w_shift_ref, w_scale_ref, w_gate_ref, out_ref):
    row = lax.broadcasted_iota(jnp.int32, (MOD_ROWS, cond_ref.shape[1]), 0)
    cond = silu(cond_ref[...].astype(F32))
    ctx = silu(ctx_ref[...].astype(F32))
    acts = jnp.where(row % 2 == 0, cond, ctx).astype(BF16)
    shifts = jnp.dot(acts, w_shift_ref[...], preferred_element_type=F32)
    scales = jnp.dot(acts, w_scale_ref[...], preferred_element_type=F32)
    gates = jnp.dot(acts, w_gate_ref[...], preferred_element_type=F32)
    out_row = lax.broadcasted_iota(jnp.int32, out_ref.shape, 0)
    out_ref[...] = jnp.where(out_row < SCALE, shifts, jnp.where(out_row < GATE, scales, gates))


def bias_kernel(pairs_ref, out_ref, *, heads):
    query = lax.broadcasted_iota(jnp.int32, (GRID_W, 2 * GRID_W), 0)
    key = lax.broadcasted_iota(jnp.int32, (GRID_W, 2 * GRID_W), 1) % GRID_W
    first = jnp.clip(query - WIN_W // 2, 0, GRID_W - WIN_W)
    inside = (key >= first) & (key < first + WIN_W)
    for h in range(heads):
        for p in range(2 * WIN_H - 2):
            row = pairs_ref[h, p : p + 1, :]
            table = pltpu.roll(
                jnp.broadcast_to(row, (GRID_W, 2 * GRID_W)),
                2 * GRID_W - (WIN_W - 1),
                1,
                stride=1,
                stride_axis=0,
            )
            out_ref[p, h * GRID_W : (h + 1) * GRID_W, :] = jnp.where(inside, table, MASKED)


def project_kernel(*refs, tp_count, sp_axis, tp_axis):
    latent_ref, context_ref, gain_ref, wq_ref, wk_ref, wv_ref = refs[:6]
    piece_refs = refs[6 : 6 + tp_count]
    q_ref, kv_ref, send_a_ref, send_b_ref, ctx_ref, resid_ref = refs[6 + tp_count : -2]
    mod_ref, normed_ref = refs[-2:]
    tokens, _ = latent_ref.shape
    cols = piece_refs[0].shape[1]
    width = wq_ref.shape[1]
    tp_index = lax.axis_index(tp_axis)
    odd = lax.axis_index(sp_axis) % 2
    for k, piece in enumerate(piece_refs):
        offset = pl.multiple_of((tp_index ^ k) * cols, 128)
        mod_ref[:, pl.ds(offset, cols)] = piece[...]
    gain = gain_ref[...].astype(F32)

    def norm(block, scale_row, shift_row):
        floats = block.astype(F32)
        inverse = lax.rsqrt(jnp.mean(floats * floats, axis=-1, keepdims=True) + EPSILON)
        factor = gain * (1.0 + mod_ref[scale_row : scale_row + 1, :])
        return (floats * inverse * factor + mod_ref[shift_row : shift_row + 1, :]).astype(BF16)

    step = 16

    def body(i, carry):
        at = pl.ds(pl.multiple_of(i * step, step), step)
        normed_ref[at, :] = norm(latent_ref[at, :], SCALE, SHIFT)
        return carry

    lax.fori_loop(0, tokens // step, body, 0, unroll=2)
    ctx_normed = norm(context_ref[...], CTX_SCALE, CTX_SHIFT)
    normed = normed_ref[...]
    kv_ref[:, :width] = jnp.dot(normed, wk_ref[...], preferred_element_type=F32).astype(BF16)
    kv_ref[:, width:] = jnp.dot(normed, wv_ref[...], preferred_element_type=F32).astype(BF16)
    halo = HALO * GRID_W
    last = tokens - halo
    send_a_ref[...] = kv_ref[pl.ds(pl.multiple_of((1 - odd) * last, 64), halo), :]
    send_b_ref[...] = kv_ref[pl.ds(pl.multiple_of(odd * last, 64), halo), :]
    query = jnp.dot(normed, wq_ref[...], preferred_element_type=F32).astype(BF16)
    q_ref[...] = query * BF16(HEAD_DIM**-0.5)
    ctx_ref[:, :width] = jnp.dot(ctx_normed, wk_ref[...], preferred_element_type=F32).astype(BF16)
    ctx_ref[:, width:] = jnp.dot(ctx_normed, wv_ref[...], preferred_element_type=F32).astype(BF16)
    resid_ref[...] = latent_ref[:, pl.ds(pl.multiple_of(tp_index * cols, 128), cols)]


def attention_kernel(*refs, sp_axis, sp_count):
    q_ref, kv_ref, recv_a_ref, recv_b_ref, table_ref = refs[:5]
    ctx_refs = refs[5:-2]
    out_ref, pad_ref = refs[-2:]
    tokens, width = q_ref.shape
    heads = width // HEAD_DIM
    rows = tokens // GRID_W
    halo = HALO * GRID_W
    sp_index = lax.axis_index(sp_axis)
    odd = sp_index % 2
    far = halo + tokens
    pad_ref[pl.ds(pl.multiple_of((1 - odd) * far, 64), halo), :] = recv_a_ref[...]
    pad_ref[pl.ds(pl.multiple_of(odd * far, 64), halo), :] = recv_b_ref[...]
    pad_ref[halo : halo + tokens, :] = kv_ref[...]
    ctx = jnp.concatenate([ref[...] for ref in ctx_refs], axis=0)
    ctx_keys, ctx_values = ctx[:, :width], ctx[:, width:]
    lane_head = lax.broadcasted_iota(jnp.int32, (1, width), 1) // HEAD_DIM
    picks = [(lane_head == h) for h in range(heads)]
    nt = (((1,), (1,)), ((), ()))
    for l in range(rows):
        at = l * GRID_W
        grid_row = sp_index * rows + l
        first = jnp.clip(grid_row - HALO, 0, sp_count * rows - WIN_H)
        start = first - sp_index * rows + HALO
        offset = first - grid_row + WIN_H - 1
        query = q_ref[at : at + GRID_W, :]
        left = jnp.concatenate([jnp.where(pick, query, BF16(0)) for pick in picks], axis=0)
        window = pl.ds(pl.multiple_of(start * GRID_W, GRID_W), WIN_H * GRID_W)
        scores = lax.dot_general(left, pad_ref[window, :width], nt, preferred_element_type=F32)
        ctx_scores = lax.dot_general(left, ctx_keys, nt, preferred_element_type=F32)
        bias = jnp.concatenate([table_ref[offset + 2 * k] for k in range(WIN_H // 2)], axis=1)
        scores = scores + bias
        highest = jnp.maximum(
            jnp.max(scores, axis=1, keepdims=True), jnp.max(ctx_scores, axis=1, keepdims=True)
        )
        win_exp = jnp.exp(scores - highest)
        ctx_exp = jnp.exp(ctx_scores - highest)
        totals = jnp.sum(win_exp, axis=1, keepdims=True) + jnp.sum(ctx_exp, axis=1, keepdims=True)
        mixed = jnp.dot(
            win_exp.astype(BF16), pad_ref[window, width:], preferred_element_type=F32
        ) + jnp.dot(ctx_exp.astype(BF16), ctx_values, preferred_element_type=F32)
        mixed = mixed * (1.0 / totals)
        result = mixed[:GRID_W]
        for h in range(1, heads):
            result = jnp.where(picks[h], mixed[h * GRID_W : (h + 1) * GRID_W], result)
        out_ref[at : at + GRID_W, :] = result.astype(BF16)


def output_kernel(*refs, masks, tp_axis):
    resid_ref, mod_ref, w_out_ref = refs[:3]
    piece_refs, out_ref = refs[3:-1], refs[-1]
    tp_index = lax.axis_index(tp_axis)
    width = piece_refs[0].shape[1]
    branch = None
    for mask, piece in zip(masks, piece_refs):
        offset = pl.multiple_of((tp_index ^ mask) * width, 128)
        part = jnp.dot(
            piece[...], w_out_ref[pl.ds(offset, width), :], preferred_element_type=F32
        )
        branch = part if branch is None else branch + part
    out_ref[...] = (resid_ref[...].astype(F32) + mod_ref[GATE : GATE + 1, :] * branch).astype(BF16)


def local(
    latent,
    conditioning,
    context,
    ctx_vector,
    w_shift,
    w_scale,
    w_gate,
    norm_gain,
    w_query,
    w_key,
    w_value,
    offset_bias,
    w_out,
):
    tokens, model = latent.shape
    cols = w_shift.shape[1]
    width = w_query.shape[1]
    heads = width // HEAD_DIM
    sp_count, tp_count = lax.axis_size("sp"), lax.axis_size("tp")
    halo = HALO * GRID_W

    partial = call(modulation_kernel, shape_of((MOD_ROWS, cols), F32))(
        conditioning[None], ctx_vector[None], w_shift, w_scale, w_gate
    )
    mod_own = total(partial, "sp")
    mod_pieces = pieces_of(mod_own, "tp")

    lanes = GRID_W - offset_bias.shape[2]
    padded = jnp.pad(offset_bias, ((0, 0), (0, 0), (0, lanes)))
    pairs = jnp.concatenate([padded[:, :-1], padded[:, 1:]], axis=2)
    table = call(
        functools.partial(bias_kernel, heads=heads),
        shape_of((2 * WIN_H - 2, heads * GRID_W, 2 * GRID_W), F32),
    )(pairs)

    query, key_value, send_a, send_b, ctx_own, resid = call(
        functools.partial(project_kernel, tp_count=tp_count, sp_axis="sp", tp_axis="tp"),
        (
            shape_of((tokens, width), BF16),
            shape_of((tokens, 2 * width), BF16),
            shape_of((halo, 2 * width), BF16),
            shape_of((halo, 2 * width), BF16),
            shape_of((context.shape[0], 2 * width), BF16),
            shape_of((tokens, cols), BF16),
        ),
        scratch=(pltpu.VMEM((MOD_ROWS, model), F32), pltpu.VMEM((tokens, model), BF16)),
    )(latent, context, norm_gain[None], w_query, w_key, w_value, *mod_pieces)

    recv_a = pairwise(send_a, "sp", 0)
    recv_b = pairwise(send_b, "sp", 1)
    ctx_all = pieces_of(ctx_own, "sp")

    attended = call(
        functools.partial(attention_kernel, sp_axis="sp", sp_count=sp_count),
        shape_of((tokens, width), BF16),
        scratch=(pltpu.VMEM((tokens + 2 * halo, 2 * width), BF16),),
    )(query, key_value, recv_a, recv_b, table, *ctx_all)

    gathered = pieces_by_bits(attended, "tp")
    return call(
        functools.partial(output_kernel, masks=[mask for mask, _ in gathered], tp_axis="tp"),
        shape_of((tokens, cols), BF16),
    )(resid, mod_own, w_out, *[piece for _, piece in gathered])


def solution(mesh):
    return jax.shard_map(
        local,
        mesh=mesh,
        in_specs=(
            P(("grp", "sp"), None),
            P(("grp", "sp")),
            P(("grp", "sp"), None),
            P("sp"),
            P("sp", "tp"),
            P("sp", "tp"),
            P("sp", "tp"),
            P(),
            P(None, "tp"),
            P(None, "tp"),
            P(None, "tp"),
            P("tp", None, None),
            P(None, "tp"),
        ),
        out_specs=P(("grp", "sp"), "tp"),
        check_vma=False,
    )
```

```python
import functools

import jax
import jax.numpy as jnp
from jax import lax
from jax.experimental import pallas as pl
from jax.experimental.pallas import tpu as pltpu
from jax.sharding import PartitionSpec as P

HEAD_DIM = 64
GRID_W = 64
WIN_H = 8
WIN_W = 16
EPSILON = 1e-06
HALO = WIN_H // 2
MASKED = -1e30
SHIFT, CTX_SHIFT, SCALE, CTX_SCALE, GATE, MOD_ROWS = 0, 1, 2, 3, 4, 8

ANY = pl.BlockSpec(memory_space=pl.ANY)
VMEM = pl.BlockSpec(memory_space=pltpu.VMEM)
F32 = jnp.float32
BF16 = jnp.bfloat16


def call(kernel, out_shape, scratch=(), vmem_mib=24, **kwargs):
    return pl.pallas_call(
        kernel,
        out_shape=out_shape,
        scratch_shapes=list(scratch),
        compiler_params=pltpu.CompilerParams(vmem_limit_bytes=vmem_mib * 2**20),
        **kwargs,
    )


def shape_of(shape, dtype):
    return jax.ShapeDtypeStruct(shape, dtype)


def digits(count):
    unit, found = 1, []
    while unit < count:
        radix = 4 if count // unit % 4 == 0 else 2
        found.append((unit, radix))
        unit *= radix
    return found


def peer(block, axis, mask):
    count = lax.axis_size(axis)
    return lax.ppermute(block, axis, [(i, i ^ mask) for i in range(count)])


def total(block, axis):
    for unit, radix in digits(lax.axis_size(axis)):
        parts = [peer(block, axis, unit * k) for k in range(1, radix)]
        for part in parts:
            block = block + part
    return block


def pieces_of(block, axis):
    pieces = [block]
    for unit, radix in digits(lax.axis_size(axis)):
        pieces = pieces + [peer(p, axis, unit * k) for k in range(1, radix) for p in pieces]
    return pieces


def pieces_by_bits(block, axis):
    pieces = [(0, block)]
    bit = lax.axis_size(axis) // 2
    while bit:
        pieces = pieces + [(mask ^ bit, peer(p, axis, bit)) for mask, p in pieces]
        bit //= 2
    return pieces


def pairwise(block, axis, first):
    count = lax.axis_size(axis)
    pairs = []
    for low in range(first, count - 1, 2):
        pairs += [(low, low + 1), (low + 1, low)]
    return lax.ppermute(block, axis, pairs)


def silu(v):
    return v / (1.0 + jnp.exp(-v))


def fetch(pairs, sems):
    copies = [
        pltpu.make_async_copy(source, target, sems.at[i]) for i, (source, target) in enumerate(pairs)
    ]
    for copy in copies:
        copy.start()
    return copies


def modulation_kernel(
    cond_hbm, ctx_hbm, w_shift_hbm, w_scale_hbm, w_gate_hbm, out_ref, *scratch
):
    cond_ref, ctx_ref, w_shift_ref, w_scale_ref, w_gate_ref, sems = scratch
    sources = (cond_hbm, ctx_hbm, w_shift_hbm, w_scale_hbm, w_gate_hbm)
    copies = fetch(list(zip(sources, scratch[:-1])), sems)
    copies[0].wait()
    copies[1].wait()
    cond = silu(cond_ref[...].astype(F32)).reshape(1, -1)
    ctx = silu(ctx_ref[...].astype(F32)).reshape(1, -1)
    row = lax.broadcasted_iota(jnp.int32, (MOD_ROWS, cond.shape[1]), 0)
    acts = jnp.where(row % 2 == 0, cond, ctx).astype(BF16)
    copies[2].wait()
    shifts = jnp.dot(acts, w_shift_ref[...], preferred_element_type=F32)
    copies[3].wait()
    scales = jnp.dot(acts, w_scale_ref[...], preferred_element_type=F32)
    copies[4].wait()
    gates = jnp.dot(acts, w_gate_ref[...], preferred_element_type=F32)
    out_row = lax.broadcasted_iota(jnp.int32, out_ref.shape, 0)
    out_ref[...] = jnp.where(out_row < SCALE, shifts, jnp.where(out_row < GATE, scales, gates))


def bias_kernel(pairs_ref, out_ref, *, heads):
    query = lax.broadcasted_iota(jnp.int32, (GRID_W, 2 * GRID_W), 0)
    key = lax.broadcasted_iota(jnp.int32, (GRID_W, 2 * GRID_W), 1) % GRID_W
    first = jnp.clip(query - WIN_W // 2, 0, GRID_W - WIN_W)
    inside = (key >= first) & (key < first + WIN_W)
    for h in range(heads):
        for p in range(2 * WIN_H - 2):
            row = pairs_ref[h, p : p + 1, :]
            table = pltpu.roll(
                jnp.broadcast_to(row, (GRID_W, 2 * GRID_W)),
                2 * GRID_W - (WIN_W - 1),
                1,
                stride=1,
                stride_axis=0,
            )
            out_ref[p, h * GRID_W : (h + 1) * GRID_W, :] = jnp.where(inside, table, MASKED)


def project_kernel(*refs, tp_count, sp_axis, tp_axis):
    latent_ref, gain_ref = refs[:2]
    sources = refs[2:6]
    piece_refs = refs[6 : 6 + tp_count]
    q_ref, kv_ref, send_a_ref, send_b_ref, ctx_ref, resid_ref = refs[6 + tp_count : -7]
    mod_ref, normed_ref = refs[-7:-5]
    context_ref, wk_ref, wv_ref, wq_ref, sems = refs[-5:]
    copies = fetch(list(zip(sources, refs[-5:-1])), sems)
    tokens, _ = latent_ref.shape
    cols = piece_refs[0].shape[1]
    width = wq_ref.shape[1]
    tp_index = lax.axis_index(tp_axis)
    odd = lax.axis_index(sp_axis) % 2
    for k, piece in enumerate(piece_refs):
        offset = pl.multiple_of((tp_index ^ k) * cols, 128)
        mod_ref[:, pl.ds(offset, cols)] = piece[...]
    gain = gain_ref[...].astype(F32)

    def norm(block, scale_row, shift_row):
        floats = block.astype(F32)
        inverse = lax.rsqrt(jnp.mean(floats * floats, axis=-1, keepdims=True) + EPSILON)
        factor = gain * (1.0 + mod_ref[scale_row : scale_row + 1, :])
        return (floats * inverse * factor + mod_ref[shift_row : shift_row + 1, :]).astype(BF16)

    step = 16

    def body(i, carry):
        at = pl.ds(pl.multiple_of(i * step, step), step)
        normed_ref[at, :] = norm(latent_ref[at, :], SCALE, SHIFT)
        return carry

    lax.fori_loop(0, tokens // step, body, 0, unroll=2)
    copies[0].wait()
    ctx_normed = norm(context_ref[...], CTX_SCALE, CTX_SHIFT)
    normed = normed_ref[...]
    copies[1].wait()
    kv_ref[:, :width] = jnp.dot(normed, wk_ref[...], preferred_element_type=F32).astype(BF16)
    copies[2].wait()
    kv_ref[:, width:] = jnp.dot(normed, wv_ref[...], preferred_element_type=F32).astype(BF16)
    halo = HALO * GRID_W
    last = tokens - halo
    send_a_ref[...] = kv_ref[pl.ds(pl.multiple_of((1 - odd) * last, 64), halo), :]
    send_b_ref[...] = kv_ref[pl.ds(pl.multiple_of(odd * last, 64), halo), :]
    copies[3].wait()
    query = jnp.dot(normed, wq_ref[...], preferred_element_type=F32).astype(BF16)
    q_ref[...] = query * BF16(HEAD_DIM**-0.5)
    ctx_ref[:, :width] = jnp.dot(ctx_normed, wk_ref[...], preferred_element_type=F32).astype(BF16)
    ctx_ref[:, width:] = jnp.dot(ctx_normed, wv_ref[...], preferred_element_type=F32).astype(BF16)
    resid_ref[...] = latent_ref[:, pl.ds(pl.multiple_of(tp_index * cols, 128), cols)]


def attention_kernel(*refs, sp_axis, sp_count):
    q_ref, kv_ref, recv_a_ref, recv_b_ref, table_ref = refs[:5]
    ctx_refs = refs[5:-2]
    out_ref, pad_ref = refs[-2:]
    tokens, width = q_ref.shape
    heads = width // HEAD_DIM
    rows = tokens // GRID_W
    halo = HALO * GRID_W
    sp_index = lax.axis_index(sp_axis)
    odd = sp_index % 2
    far = halo + tokens
    pad_ref[pl.ds(pl.multiple_of((1 - odd) * far, 64), halo), :] = recv_a_ref[...]
    pad_ref[pl.ds(pl.multiple_of(odd * far, 64), halo), :] = recv_b_ref[...]
    pad_ref[halo : halo + tokens, :] = kv_ref[...]
    ctx = jnp.concatenate([ref[...] for ref in ctx_refs], axis=0)
    ctx_keys, ctx_values = ctx[:, :width], ctx[:, width:]
    lane_head = lax.broadcasted_iota(jnp.int32, (1, width), 1) // HEAD_DIM
    picks = [(lane_head == h) for h in range(heads)]
    nt = (((1,), (1,)), ((), ()))
    for l in range(rows):
        at = l * GRID_W
        grid_row = sp_index * rows + l
        first = jnp.clip(grid_row - HALO, 0, sp_count * rows - WIN_H)
        start = first - sp_index * rows + HALO
        offset = first - grid_row + WIN_H - 1
        query = q_ref[at : at + GRID_W, :]
        left = jnp.concatenate([jnp.where(pick, query, BF16(0)) for pick in picks], axis=0)
        window = pl.ds(pl.multiple_of(start * GRID_W, GRID_W), WIN_H * GRID_W)
        scores = lax.dot_general(left, pad_ref[window, :width], nt, preferred_element_type=F32)
        ctx_scores = lax.dot_general(left, ctx_keys, nt, preferred_element_type=F32)
        bias = jnp.concatenate([table_ref[offset + 2 * k] for k in range(WIN_H // 2)], axis=1)
        scores = scores + bias
        highest = jnp.maximum(
            jnp.max(scores, axis=1, keepdims=True), jnp.max(ctx_scores, axis=1, keepdims=True)
        )
        win_exp = jnp.exp(scores - highest)
        ctx_exp = jnp.exp(ctx_scores - highest)
        totals = jnp.sum(win_exp, axis=1, keepdims=True) + jnp.sum(ctx_exp, axis=1, keepdims=True)
        mixed = jnp.dot(
            win_exp.astype(BF16), pad_ref[window, width:], preferred_element_type=F32
        ) + jnp.dot(ctx_exp.astype(BF16), ctx_values, preferred_element_type=F32)
        mixed = mixed * (1.0 / totals)
        result = mixed[:GRID_W]
        for h in range(1, heads):
            result = jnp.where(picks[h], mixed[h * GRID_W : (h + 1) * GRID_W], result)
        out_ref[at : at + GRID_W, :] = result.astype(BF16)


def output_kernel(*refs, masks, tp_axis):
    resid_ref, mod_ref, w_out_ref = refs[:3]
    piece_refs, out_ref = refs[3:-1], refs[-1]
    tp_index = lax.axis_index(tp_axis)
    width = piece_refs[0].shape[1]
    branch = None
    for mask, piece in zip(masks, piece_refs):
        offset = pl.multiple_of((tp_index ^ mask) * width, 128)
        part = jnp.dot(
            piece[...], w_out_ref[pl.ds(offset, width), :], preferred_element_type=F32
        )
        branch = part if branch is None else branch + part
    out_ref[...] = (resid_ref[...].astype(F32) + mod_ref[GATE : GATE + 1, :] * branch).astype(BF16)


def local(
    latent,
    conditioning,
    context,
    ctx_vector,
    w_shift,
    w_scale,
    w_gate,
    norm_gain,
    w_query,
    w_key,
    w_value,
    offset_bias,
    w_out,
):
    tokens, model = latent.shape
    cols = w_shift.shape[1]
    width = w_query.shape[1]
    heads = width // HEAD_DIM
    sp_count, tp_count = lax.axis_size("sp"), lax.axis_size("tp")
    halo = HALO * GRID_W

    mod_inputs = (conditioning, ctx_vector, w_shift, w_scale, w_gate)
    partial = call(
        modulation_kernel,
        shape_of((MOD_ROWS, cols), F32),
        scratch=[pltpu.VMEM(a.shape, a.dtype) for a in mod_inputs] + [pltpu.SemaphoreType.DMA((5,))],
        in_specs=[ANY] * 5,
    )(*mod_inputs)
    mod_own = total(partial, "sp")
    mod_pieces = pieces_of(mod_own, "tp")

    lanes = GRID_W - offset_bias.shape[2]
    padded = jnp.pad(offset_bias, ((0, 0), (0, 0), (0, lanes)))
    pairs = jnp.concatenate([padded[:, :-1], padded[:, 1:]], axis=2)
    table = call(
        functools.partial(bias_kernel, heads=heads),
        shape_of((2 * WIN_H - 2, heads * GRID_W, 2 * GRID_W), F32),
    )(pairs)

    fetched = (context, w_key, w_value, w_query)
    query, key_value, send_a, send_b, ctx_own, resid = call(
        functools.partial(project_kernel, tp_count=tp_count, sp_axis="sp", tp_axis="tp"),
        (
            shape_of((tokens, width), BF16),
            shape_of((tokens, 2 * width), BF16),
            shape_of((halo, 2 * width), BF16),
            shape_of((halo, 2 * width), BF16),
            shape_of((context.shape[0], 2 * width), BF16),
            shape_of((tokens, cols), BF16),
        ),
        scratch=[pltpu.VMEM((MOD_ROWS, model), F32), pltpu.VMEM((tokens, model), BF16)]
        + [pltpu.VMEM(a.shape, a.dtype) for a in fetched]
        + [pltpu.SemaphoreType.DMA((4,))],
        in_specs=[VMEM] * 2 + [ANY] * 4 + [VMEM] * tp_count,
    )(latent, norm_gain[None], *fetched, *mod_pieces)

    recv_a = pairwise(send_a, "sp", 0)
    recv_b = pairwise(send_b, "sp", 1)
    ctx_all = pieces_of(ctx_own, "sp")

    attended = call(
        functools.partial(attention_kernel, sp_axis="sp", sp_count=sp_count),
        shape_of((tokens, width), BF16),
        scratch=(pltpu.VMEM((tokens + 2 * halo, 2 * width), BF16),),
    )(query, key_value, recv_a, recv_b, table, *ctx_all)

    gathered = pieces_by_bits(attended, "tp")
    return call(
        functools.partial(output_kernel, masks=[mask for mask, _ in gathered], tp_axis="tp"),
        shape_of((tokens, cols), BF16),
    )(resid, mod_own, w_out, *[piece for _, piece in gathered])


def solution(mesh):
    return jax.shard_map(
        local,
        mesh=mesh,
        in_specs=(
            P(("grp", "sp"), None),
            P(("grp", "sp")),
            P(("grp", "sp"), None),
            P("sp"),
            P("sp", "tp"),
            P("sp", "tp"),
            P("sp", "tp"),
            P(),
            P(None, "tp"),
            P(None, "tp"),
            P(None, "tp"),
            P("tp", None, None),
            P(None, "tp"),
        ),
        out_specs=P(("grp", "sp"), "tp"),
        check_vma=False,
    )
```

```python
import functools

import jax
import jax.numpy as jnp
from jax import lax
from jax.experimental import pallas as pl
from jax.experimental.pallas import tpu as pltpu
from jax.sharding import PartitionSpec as P

HEAD_DIM = 64
GRID_W = 64
WIN_H = 8
WIN_W = 16
EPSILON = 1e-06
HALO = WIN_H // 2
MASKED = -1e30
SHIFT, CTX_SHIFT, SCALE, CTX_SCALE, GATE, MOD_ROWS = 0, 1, 2, 3, 4, 8

HBM = pl.BlockSpec(memory_space=pltpu.HBM)
VMEM = pl.BlockSpec(memory_space=pltpu.VMEM)
F32 = jnp.float32
BF16 = jnp.bfloat16


def call(kernel, out_shape, scratch=(), vmem_mib=24, **kwargs):
    return pl.pallas_call(
        kernel,
        out_shape=out_shape,
        scratch_shapes=list(scratch),
        compiler_params=pltpu.CompilerParams(vmem_limit_bytes=vmem_mib * 2**20),
        **kwargs,
    )


def in_hbm(arrays):
    return [pltpu.with_memory_space_constraint(a, pltpu.HBM) for a in arrays]


def shape_of(shape, dtype):
    return jax.ShapeDtypeStruct(shape, dtype)


def digits(count):
    unit, found = 1, []
    while unit < count:
        radix = 4 if count // unit % 4 == 0 else 2
        found.append((unit, radix))
        unit *= radix
    return found


def peer(block, axis, mask):
    count = lax.axis_size(axis)
    return lax.ppermute(block, axis, [(i, i ^ mask) for i in range(count)])


def total(block, axis):
    for unit, radix in digits(lax.axis_size(axis)):
        parts = [peer(block, axis, unit * k) for k in range(1, radix)]
        for part in parts:
            block = block + part
    return block


def pieces_of(block, axis):
    pieces = [block]
    for unit, radix in digits(lax.axis_size(axis)):
        pieces = pieces + [peer(p, axis, unit * k) for k in range(1, radix) for p in pieces]
    return pieces


def pieces_by_bits(block, axis):
    pieces = [(0, block)]
    bit = lax.axis_size(axis) // 2
    while bit:
        pieces = pieces + [(mask ^ bit, peer(p, axis, bit)) for mask, p in pieces]
        bit //= 2
    return pieces


def pairwise(block, axis, first):
    count = lax.axis_size(axis)
    pairs = []
    for low in range(first, count - 1, 2):
        pairs += [(low, low + 1), (low + 1, low)]
    return lax.ppermute(block, axis, pairs)


def silu(v):
    return v / (1.0 + jnp.exp(-v))


def fetch(pairs, sems):
    copies = [
        pltpu.make_async_copy(source, target, sems.at[i]) for i, (source, target) in enumerate(pairs)
    ]
    for copy in copies:
        copy.start()
    return copies


def modulation_kernel(
    cond_hbm, ctx_hbm, w_shift_hbm, w_scale_hbm, w_gate_hbm, out_ref, *scratch
):
    cond_ref, ctx_ref, w_shift_ref, w_scale_ref, w_gate_ref, sems = scratch
    sources = (cond_hbm, ctx_hbm, w_shift_hbm, w_scale_hbm, w_gate_hbm)
    copies = fetch(list(zip(sources, scratch[:-1])), sems)
    copies[0].wait()
    copies[1].wait()
    cond = silu(cond_ref[...].astype(F32)).reshape(1, -1)
    ctx = silu(ctx_ref[...].astype(F32)).reshape(1, -1)
    row = lax.broadcasted_iota(jnp.int32, (MOD_ROWS, cond.shape[1]), 0)
    acts = jnp.where(row % 2 == 0, cond, ctx).astype(BF16)
    copies[2].wait()
    shifts = jnp.dot(acts, w_shift_ref[...], preferred_element_type=F32)
    copies[3].wait()
    scales = jnp.dot(acts, w_scale_ref[...], preferred_element_type=F32)
    copies[4].wait()
    gates = jnp.dot(acts, w_gate_ref[...], preferred_element_type=F32)
    out_row = lax.broadcasted_iota(jnp.int32, out_ref.shape, 0)
    out_ref[...] = jnp.where(out_row < SCALE, shifts, jnp.where(out_row < GATE, scales, gates))


def bias_kernel(pairs_ref, out_ref, *, heads):
    query = lax.broadcasted_iota(jnp.int32, (GRID_W, 2 * GRID_W), 0)
    key = lax.broadcasted_iota(jnp.int32, (GRID_W, 2 * GRID_W), 1) % GRID_W
    first = jnp.clip(query - WIN_W // 2, 0, GRID_W - WIN_W)
    inside = (key >= first) & (key < first + WIN_W)
    for h in range(heads):
        for p in range(2 * WIN_H - 2):
            row = pairs_ref[h, p : p + 1, :]
            table = pltpu.roll(
                jnp.broadcast_to(row, (GRID_W, 2 * GRID_W)),
                2 * GRID_W - (WIN_W - 1),
                1,
                stride=1,
                stride_axis=0,
            )
            out_ref[p, h * GRID_W : (h + 1) * GRID_W, :] = jnp.where(inside, table, MASKED)


def project_kernel(*refs, tp_count, sp_axis, tp_axis):
    latent_ref, gain_ref = refs[:2]
    sources = refs[2:6]
    piece_refs = refs[6 : 6 + tp_count]
    q_ref, kv_ref, send_a_ref, send_b_ref, ctx_ref, resid_ref = refs[6 + tp_count : -7]
    mod_ref, normed_ref = refs[-7:-5]
    context_ref, wk_ref, wv_ref, wq_ref, sems = refs[-5:]
    copies = fetch(list(zip(sources, refs[-5:-1])), sems)
    tokens, _ = latent_ref.shape
    cols = piece_refs[0].shape[1]
    width = wq_ref.shape[1]
    tp_index = lax.axis_index(tp_axis)
    odd = lax.axis_index(sp_axis) % 2
    for k, piece in enumerate(piece_refs):
        offset = pl.multiple_of((tp_index ^ k) * cols, 128)
        mod_ref[:, pl.ds(offset, cols)] = piece[...]
    gain = gain_ref[...].astype(F32)

    def norm(block, scale_row, shift_row):
        floats = block.astype(F32)
        inverse = lax.rsqrt(jnp.mean(floats * floats, axis=-1, keepdims=True) + EPSILON)
        factor = gain * (1.0 + mod_ref[scale_row : scale_row + 1, :])
        return (floats * inverse * factor + mod_ref[shift_row : shift_row + 1, :]).astype(BF16)

    step = 16

    def body(i, carry):
        at = pl.ds(pl.multiple_of(i * step, step), step)
        normed_ref[at, :] = norm(latent_ref[at, :], SCALE, SHIFT)
        return carry

    lax.fori_loop(0, tokens // step, body, 0, unroll=2)
    copies[0].wait()
    ctx_normed = norm(context_ref[...], CTX_SCALE, CTX_SHIFT)
    normed = normed_ref[...]
    copies[1].wait()
    kv_ref[:, :width] = jnp.dot(normed, wk_ref[...], preferred_element_type=F32).astype(BF16)
    copies[2].wait()
    kv_ref[:, width:] = jnp.dot(normed, wv_ref[...], preferred_element_type=F32).astype(BF16)
    halo = HALO * GRID_W
    last = tokens - halo
    send_a_ref[...] = kv_ref[pl.ds(pl.multiple_of((1 - odd) * last, 64), halo), :]
    send_b_ref[...] = kv_ref[pl.ds(pl.multiple_of(odd * last, 64), halo), :]
    copies[3].wait()
    query = jnp.dot(normed, wq_ref[...], preferred_element_type=F32).astype(BF16)
    q_ref[...] = query * BF16(HEAD_DIM**-0.5)
    ctx_ref[:, :width] = jnp.dot(ctx_normed, wk_ref[...], preferred_element_type=F32).astype(BF16)
    ctx_ref[:, width:] = jnp.dot(ctx_normed, wv_ref[...], preferred_element_type=F32).astype(BF16)
    resid_ref[...] = latent_ref[:, pl.ds(pl.multiple_of(tp_index * cols, 128), cols)]


def attention_kernel(*refs, sp_axis, sp_count):
    q_ref, kv_ref, recv_a_ref, recv_b_ref, table_ref = refs[:5]
    ctx_refs = refs[5:-2]
    out_ref, pad_ref = refs[-2:]
    tokens, width = q_ref.shape
    heads = width // HEAD_DIM
    rows = tokens // GRID_W
    halo = HALO * GRID_W
    sp_index = lax.axis_index(sp_axis)
    odd = sp_index % 2
    far = halo + tokens
    pad_ref[pl.ds(pl.multiple_of((1 - odd) * far, 64), halo), :] = recv_a_ref[...]
    pad_ref[pl.ds(pl.multiple_of(odd * far, 64), halo), :] = recv_b_ref[...]
    pad_ref[halo : halo + tokens, :] = kv_ref[...]
    ctx = jnp.concatenate([ref[...] for ref in ctx_refs], axis=0)
    ctx_keys, ctx_values = ctx[:, :width], ctx[:, width:]
    lane_head = lax.broadcasted_iota(jnp.int32, (1, width), 1) // HEAD_DIM
    picks = [(lane_head == h) for h in range(heads)]
    nt = (((1,), (1,)), ((), ()))
    for l in range(rows):
        at = l * GRID_W
        grid_row = sp_index * rows + l
        first = jnp.clip(grid_row - HALO, 0, sp_count * rows - WIN_H)
        start = first - sp_index * rows + HALO
        offset = first - grid_row + WIN_H - 1
        query = q_ref[at : at + GRID_W, :]
        left = jnp.concatenate([jnp.where(pick, query, BF16(0)) for pick in picks], axis=0)
        window = pl.ds(pl.multiple_of(start * GRID_W, GRID_W), WIN_H * GRID_W)
        scores = lax.dot_general(left, pad_ref[window, :width], nt, preferred_element_type=F32)
        ctx_scores = lax.dot_general(left, ctx_keys, nt, preferred_element_type=F32)
        bias = jnp.concatenate([table_ref[offset + 2 * k] for k in range(WIN_H // 2)], axis=1)
        scores = scores + bias
        highest = jnp.maximum(
            jnp.max(scores, axis=1, keepdims=True), jnp.max(ctx_scores, axis=1, keepdims=True)
        )
        win_exp = jnp.exp(scores - highest)
        ctx_exp = jnp.exp(ctx_scores - highest)
        totals = jnp.sum(win_exp, axis=1, keepdims=True) + jnp.sum(ctx_exp, axis=1, keepdims=True)
        mixed = jnp.dot(
            win_exp.astype(BF16), pad_ref[window, width:], preferred_element_type=F32
        ) + jnp.dot(ctx_exp.astype(BF16), ctx_values, preferred_element_type=F32)
        mixed = mixed * (1.0 / totals)
        result = mixed[:GRID_W]
        for h in range(1, heads):
            result = jnp.where(picks[h], mixed[h * GRID_W : (h + 1) * GRID_W], result)
        out_ref[at : at + GRID_W, :] = result.astype(BF16)


def output_kernel(*refs, masks, tp_axis):
    resid_ref, mod_ref, w_out_ref = refs[:3]
    piece_refs, out_ref = refs[3:-1], refs[-1]
    tp_index = lax.axis_index(tp_axis)
    width = piece_refs[0].shape[1]
    branch = None
    for mask, piece in zip(masks, piece_refs):
        offset = pl.multiple_of((tp_index ^ mask) * width, 128)
        part = jnp.dot(
            piece[...], w_out_ref[pl.ds(offset, width), :], preferred_element_type=F32
        )
        branch = part if branch is None else branch + part
    out_ref[...] = (resid_ref[...].astype(F32) + mod_ref[GATE : GATE + 1, :] * branch).astype(BF16)


def local(
    latent,
    conditioning,
    context,
    ctx_vector,
    w_shift,
    w_scale,
    w_gate,
    norm_gain,
    w_query,
    w_key,
    w_value,
    offset_bias,
    w_out,
):
    tokens, model = latent.shape
    cols = w_shift.shape[1]
    width = w_query.shape[1]
    heads = width // HEAD_DIM
    sp_count, tp_count = lax.axis_size("sp"), lax.axis_size("tp")
    halo = HALO * GRID_W

    mod_inputs = (conditioning, ctx_vector, w_shift, w_scale, w_gate)
    partial = call(
        modulation_kernel,
        shape_of((MOD_ROWS, cols), F32),
        scratch=[pltpu.VMEM(a.shape, a.dtype) for a in mod_inputs] + [pltpu.SemaphoreType.DMA((5,))],
        in_specs=[HBM] * 5,
    )(*in_hbm(mod_inputs))
    mod_own = total(partial, "sp")
    mod_pieces = pieces_of(mod_own, "tp")

    lanes = GRID_W - offset_bias.shape[2]
    padded = jnp.pad(offset_bias, ((0, 0), (0, 0), (0, lanes)))
    pairs = jnp.concatenate([padded[:, :-1], padded[:, 1:]], axis=2)
    table = call(
        functools.partial(bias_kernel, heads=heads),
        shape_of((2 * WIN_H - 2, heads * GRID_W, 2 * GRID_W), F32),
    )(pairs)

    fetched = (context, w_key, w_value, w_query)
    query, key_value, send_a, send_b, ctx_own, resid = call(
        functools.partial(project_kernel, tp_count=tp_count, sp_axis="sp", tp_axis="tp"),
        (
            shape_of((tokens, width), BF16),
            shape_of((tokens, 2 * width), BF16),
            shape_of((halo, 2 * width), BF16),
            shape_of((halo, 2 * width), BF16),
            shape_of((context.shape[0], 2 * width), BF16),
            shape_of((tokens, cols), BF16),
        ),
        scratch=[pltpu.VMEM((MOD_ROWS, model), F32), pltpu.VMEM((tokens, model), BF16)]
        + [pltpu.VMEM(a.shape, a.dtype) for a in fetched]
        + [pltpu.SemaphoreType.DMA((4,))],
        in_specs=[VMEM] * 2 + [HBM] * 4 + [VMEM] * tp_count,
    )(latent, norm_gain[None], *in_hbm(fetched), *mod_pieces)

    recv_a = pairwise(send_a, "sp", 0)
    recv_b = pairwise(send_b, "sp", 1)
    ctx_all = pieces_of(ctx_own, "sp")

    attended = call(
        functools.partial(attention_kernel, sp_axis="sp", sp_count=sp_count),
        shape_of((tokens, width), BF16),
        scratch=(pltpu.VMEM((tokens + 2 * halo, 2 * width), BF16),),
    )(query, key_value, recv_a, recv_b, table, *ctx_all)

    gathered = pieces_by_bits(attended, "tp")
    return call(
        functools.partial(output_kernel, masks=[mask for mask, _ in gathered], tp_axis="tp"),
        shape_of((tokens, cols), BF16),
    )(resid, mod_own, w_out, *[piece for _, piece in gathered])


def solution(mesh):
    return jax.shard_map(
        local,
        mesh=mesh,
        in_specs=(
            P(("grp", "sp"), None),
            P(("grp", "sp")),
            P(("grp", "sp"), None),
            P("sp"),
            P("sp", "tp"),
            P("sp", "tp"),
            P("sp", "tp"),
            P(),
            P(None, "tp"),
            P(None, "tp"),
            P(None, "tp"),
            P("tp", None, None),
            P(None, "tp"),
        ),
        out_specs=P(("grp", "sp"), "tp"),
        check_vma=False,
    )
```

```python
import functools

import jax
import jax.numpy as jnp
from jax import lax
from jax.experimental import pallas as pl
from jax.experimental.pallas import tpu as pltpu
from jax.sharding import PartitionSpec as P

HEAD_DIM = 64
GRID_W = 64
WIN_H = 8
WIN_W = 16
EPSILON = 1e-06
HALO = WIN_H // 2
MASKED = -1e30
SHIFT, CTX_SHIFT, SCALE, CTX_SCALE, GATE, MOD_ROWS = 0, 1, 2, 3, 4, 8

HBM = pl.BlockSpec(memory_space=pltpu.HBM)
VMEM = pl.BlockSpec(memory_space=pltpu.VMEM)
F32 = jnp.float32
BF16 = jnp.bfloat16


def call(kernel, out_shape, scratch=(), vmem_mib=24, **kwargs):
    return pl.pallas_call(
        kernel,
        out_shape=out_shape,
        scratch_shapes=list(scratch),
        compiler_params=pltpu.CompilerParams(vmem_limit_bytes=vmem_mib * 2**20),
        **kwargs,
    )


def in_hbm(arrays):
    return [pltpu.with_memory_space_constraint(a, pltpu.HBM) for a in arrays]


def shape_of(shape, dtype):
    return jax.ShapeDtypeStruct(shape, dtype)


def digits(count):
    unit, found = 1, []
    while unit < count:
        radix = 4 if count // unit % 4 == 0 else 2
        found.append((unit, radix))
        unit *= radix
    return found


def peer(block, axis, mask):
    count = lax.axis_size(axis)
    return lax.ppermute(block, axis, [(i, i ^ mask) for i in range(count)])


def joined(parts):
    sums = None
    for part in parts:
        rows = part[:MOD_ROWS].astype(F32) + part[MOD_ROWS : 2 * MOD_ROWS].astype(F32)
        sums = rows if sums is None else sums + rows
    return sums, jnp.concatenate([part[2 * MOD_ROWS :] for part in parts], axis=0)


def total_and_context(block, axis):
    steps = digits(lax.axis_size(axis))
    for i, (unit, radix) in enumerate(steps):
        far_first = [peer(block, axis, unit * k) for k in reversed(range(1, radix))]
        sums, context = joined([block] + far_first)
        if i + 1 < len(steps):
            high = lax.reduce_precision(sums, 8, 7)
            block = jnp.concatenate([high, sums - high], axis=0).astype(BF16)
            block = jnp.concatenate([block, context], axis=0)
    return sums, context


def pieces_of(block, axis):
    pieces = [block]
    for unit, radix in digits(lax.axis_size(axis)):
        pieces = pieces + [peer(p, axis, unit * k) for k in range(1, radix) for p in pieces]
    return pieces


def pieces_by_bits(block, axis):
    pieces = [(0, block)]
    bit = lax.axis_size(axis) // 2
    while bit:
        pieces = pieces + [(mask ^ bit, peer(p, axis, bit)) for mask, p in pieces]
        bit //= 2
    return pieces


def pairwise(block, axis, first):
    count = lax.axis_size(axis)
    pairs = []
    for low in range(first, count - 1, 2):
        pairs += [(low, low + 1), (low + 1, low)]
    return lax.ppermute(block, axis, pairs)


def silu(v):
    return v / (1.0 + jnp.exp(-v))


def fetch(pairs, sems):
    copies = [
        pltpu.make_async_copy(source, target, sems.at[i]) for i, (source, target) in enumerate(pairs)
    ]
    for copy in copies:
        copy.start()
    return copies


def modulation_kernel(
    cond_hbm, ctx_hbm, w_shift_hbm, w_scale_hbm, w_gate_hbm, context_hbm, out_ref, *scratch
):
    cond_ref, ctx_ref, w_shift_ref, w_scale_ref, w_gate_ref, context_ref, sems = scratch
    cols = w_shift_ref.shape[1]
    own = pl.ds(pl.multiple_of(lax.axis_index("tp") * cols, 128), cols)
    sources = (cond_hbm, ctx_hbm, w_shift_hbm, w_scale_hbm, w_gate_hbm, context_hbm.at[:, own])
    copies = fetch(list(zip(sources, scratch[:-1])), sems)
    copies[0].wait()
    copies[1].wait()
    cond = silu(cond_ref[...].astype(F32)).reshape(1, -1)
    ctx = silu(ctx_ref[...].astype(F32)).reshape(1, -1)
    row = lax.broadcasted_iota(jnp.int32, (MOD_ROWS, cond.shape[1]), 0)
    acts = jnp.where(row % 2 == 0, cond, ctx).astype(BF16)
    copies[2].wait()
    shifts = jnp.dot(acts, w_shift_ref[...], preferred_element_type=F32)
    copies[3].wait()
    scales = jnp.dot(acts, w_scale_ref[...], preferred_element_type=F32)
    copies[4].wait()
    gates = jnp.dot(acts, w_gate_ref[...], preferred_element_type=F32)
    out_row = lax.broadcasted_iota(jnp.int32, shifts.shape, 0)
    sums = jnp.where(out_row < SCALE, shifts, jnp.where(out_row < GATE, scales, gates))
    high = sums.astype(BF16).astype(F32)
    out_ref[: 2 * MOD_ROWS, :] = jnp.concatenate([high, sums - high], axis=0).astype(BF16)
    copies[5].wait()
    out_ref[2 * MOD_ROWS :, :] = context_ref[...]


def bias_kernel(pairs_ref, out_ref, *, heads):
    query = lax.broadcasted_iota(jnp.int32, (GRID_W, 2 * GRID_W), 0)
    key = lax.broadcasted_iota(jnp.int32, (GRID_W, 2 * GRID_W), 1) % GRID_W
    first = jnp.clip(query - WIN_W // 2, 0, GRID_W - WIN_W)
    inside = (key >= first) & (key < first + WIN_W)
    for h in range(heads):
        for p in range(2 * WIN_H - 2):
            row = pairs_ref[h, p : p + 1, :]
            table = pltpu.roll(
                jnp.broadcast_to(row, (GRID_W, 2 * GRID_W)),
                2 * GRID_W - (WIN_W - 1),
                1,
                stride=1,
                stride_axis=0,
            )
            out_ref[p, h * GRID_W : (h + 1) * GRID_W, :] = jnp.where(inside, table, MASKED)


def inverse_rms(floats):
    return lax.rsqrt(jnp.mean(floats * floats, axis=-1, keepdims=True) + EPSILON)


def send_halo(kv_ref, send_a_ref, send_b_ref):
    halo = HALO * GRID_W
    last = kv_ref.shape[0] - halo
    odd = lax.axis_index("sp") % 2
    send_a_ref[...] = kv_ref[pl.ds(pl.multiple_of((1 - odd) * last, GRID_W), halo), :]
    send_b_ref[...] = kv_ref[pl.ds(pl.multiple_of(odd * last, GRID_W), halo), :]


def norm_kernel(*refs, tp_count, chunks):
    latent_ref, gain_hbm, wk_hbm, wv_hbm = refs[:4]
    piece_refs = refs[4 : 4 + tp_count]
    outs = refs[4 + tp_count : -4]
    normed_ref, kv_ref, send_a_ref, send_b_ref, mod_ref, gain_out_ref = outs[:6]
    weight_refs = outs[6:]
    gain_ref, factor_ref, offset_ref, sems = refs[-4:]
    tokens, _ = latent_ref.shape
    cols = piece_refs[0].shape[1]
    each = weight_refs[0].shape[1] // 2
    pairs = [(gain_hbm, gain_ref)]
    for c, weight in enumerate(weight_refs):
        at = pl.ds(c * each, each)
        pairs += [(wk_hbm.at[:, at], weight.at[:, :each]), (wv_hbm.at[:, at], weight.at[:, each:])]
    copies = fetch(pairs, sems)
    tp_index = lax.axis_index("tp")
    for k, piece in enumerate(piece_refs):
        offset = pl.multiple_of((tp_index ^ k) * cols, 128)
        mod_ref[:, pl.ds(offset, cols)] = piece[...]
    copies[0].wait()
    gain = gain_ref[...].astype(F32).reshape(1, -1)
    gain_out_ref[...] = jnp.broadcast_to(gain, gain_out_ref.shape)
    factor_ref[...] = jnp.broadcast_to(gain * (1.0 + mod_ref[SCALE : SCALE + 1, :]), factor_ref.shape)
    offset_ref[...] = jnp.broadcast_to(mod_ref[SHIFT : SHIFT + 1, :], offset_ref.shape)
    step = 16

    def body(i, carry):
        at = pl.ds(pl.multiple_of(i * step, step), step)
        floats = latent_ref[at, :].astype(F32)
        scaled = (floats * inverse_rms(floats)).reshape(step // 8, 8, -1)
        result = scaled * factor_ref[...][None] + offset_ref[...][None]
        normed_ref[at, :] = result.reshape(step, -1).astype(BF16)
        return carry

    lax.fori_loop(0, tokens // step, body, 0, unroll=2)
    copies[1].wait()
    copies[2].wait()
    kv_ref[...] = jnp.dot(
        normed_ref[...], weight_refs[0][...], preferred_element_type=F32
    ).astype(BF16)
    send_halo(kv_ref, send_a_ref, send_b_ref)
    for copy in copies[3:]:
        copy.wait()


def chunk_kernel(normed_ref, weight_ref, kv_ref, send_a_ref, send_b_ref):
    kv_ref[...] = jnp.dot(
        normed_ref[...], weight_ref[...], preferred_element_type=F32
    ).astype(BF16)
    send_halo(kv_ref, send_a_ref, send_b_ref)


def query_kernel(normed_ref, wq_ref, latent_ref, q_ref, resid_ref):
    cols = resid_ref.shape[1]
    query = jnp.dot(normed_ref[...], wq_ref[...], preferred_element_type=F32).astype(BF16)
    q_ref[...] = query * BF16(HEAD_DIM**-0.5)
    own = pl.ds(pl.multiple_of(lax.axis_index("tp") * cols, 128), cols)
    resid_ref[...] = latent_ref[:, own]


def context_kernel(*refs, masks, chunks):
    mod_ref, gain_ref = refs[:2]
    piece_refs = refs[2 : 2 + len(masks)]
    weight_refs = refs[2 + len(masks) : 2 + len(masks) + chunks]
    out_refs, whole_ref = refs[2 + len(masks) + chunks : -1], refs[-1]
    cols = piece_refs[0].shape[1]
    tp_index = lax.axis_index("tp")
    for mask, piece in zip(masks, piece_refs):
        whole_ref[:, pl.ds(pl.multiple_of((tp_index ^ mask) * cols, 128), cols)] = piece[...]
    floats = whole_ref[...].astype(F32)
    factor = gain_ref[0:1, :] * (1.0 + mod_ref[CTX_SCALE : CTX_SCALE + 1, :])
    shift = mod_ref[CTX_SHIFT : CTX_SHIFT + 1, :]
    normed = (floats * inverse_rms(floats) * factor + shift).astype(BF16)
    for weight, out in zip(weight_refs, out_refs):
        out[...] = jnp.dot(normed, weight[...], preferred_element_type=F32).astype(BF16)


def attention_kernel(
    q_ref, kv_ref, recv_a_ref, recv_b_ref, table_ref, ctx_ref, out_ref, pad_ref, *, chunk, sp_count
):
    tokens, width = out_ref.shape
    heads = width // HEAD_DIM
    rows = tokens // GRID_W
    halo = HALO * GRID_W
    sp_index = lax.axis_index("sp")
    odd = sp_index % 2
    far = halo + tokens
    pad_ref[pl.ds(pl.multiple_of((1 - odd) * far, GRID_W), halo), :] = recv_a_ref[...]
    pad_ref[pl.ds(pl.multiple_of(odd * far, GRID_W), halo), :] = recv_b_ref[...]
    pad_ref[halo : halo + tokens, :] = kv_ref[...]
    ctx_keys, ctx_values = ctx_ref[:, :width], ctx_ref[:, width:]
    lane_head = lax.broadcasted_iota(jnp.int32, (1, width), 1) // HEAD_DIM
    picks = [(lane_head == h) for h in range(heads)]
    table_rows = slice(chunk * heads * GRID_W, (chunk + 1) * heads * GRID_W)
    nt = (((1,), (1,)), ((), ()))
    for l in range(rows):
        at = l * GRID_W
        grid_row = sp_index * rows + l
        first = jnp.clip(grid_row - HALO, 0, sp_count * rows - WIN_H)
        start = first - sp_index * rows + HALO
        offset = first - grid_row + WIN_H - 1
        query = q_ref[at : at + GRID_W, chunk * width : (chunk + 1) * width]
        left = jnp.concatenate([jnp.where(pick, query, BF16(0)) for pick in picks], axis=0)
        window = pl.ds(pl.multiple_of(start * GRID_W, GRID_W), WIN_H * GRID_W)
        scores = lax.dot_general(left, pad_ref[window, :width], nt, preferred_element_type=F32)
        ctx_scores = lax.dot_general(left, ctx_keys, nt, preferred_element_type=F32)
        bias = jnp.concatenate(
            [table_ref[offset + 2 * k, table_rows, :] for k in range(WIN_H // 2)], axis=1
        )
        scores = scores + bias
        highest = jnp.maximum(
            jnp.max(scores, axis=1, keepdims=True), jnp.max(ctx_scores, axis=1, keepdims=True)
        )
        win_exp = jnp.exp(scores - highest)
        ctx_exp = jnp.exp(ctx_scores - highest)
        totals = jnp.sum(win_exp, axis=1, keepdims=True) + jnp.sum(ctx_exp, axis=1, keepdims=True)
        mixed = jnp.dot(
            win_exp.astype(BF16), pad_ref[window, width:], preferred_element_type=F32
        ) + jnp.dot(ctx_exp.astype(BF16), ctx_values, preferred_element_type=F32)
        mixed = mixed * (1.0 / totals)
        result = mixed[:GRID_W]
        for h in range(1, heads):
            result = jnp.where(picks[h], mixed[h * GRID_W : (h + 1) * GRID_W], result)
        out_ref[at : at + GRID_W, :] = result.astype(BF16)


def output_kernel(*refs, masks, chunks):
    resid_ref, mod_ref, w_out_ref = refs[:3]
    piece_refs, out_ref = refs[3:-1], refs[-1]
    tp_index = lax.axis_index("tp")
    count = len(masks)
    width = chunks * piece_refs[0].shape[1]
    branch = None
    for i, mask in enumerate(masks):
        offset = pl.multiple_of((tp_index ^ mask) * width, 128)
        piece = jnp.concatenate([piece_refs[c * count + i][...] for c in range(chunks)], axis=1)
        part = jnp.dot(piece, w_out_ref[pl.ds(offset, width), :], preferred_element_type=F32)
        branch = part if branch is None else branch + part
    out_ref[...] = (resid_ref[...].astype(F32) + mod_ref[GATE : GATE + 1, :] * branch).astype(BF16)


def local(
    latent,
    conditioning,
    context,
    ctx_vector,
    w_shift,
    w_scale,
    w_gate,
    norm_gain,
    w_query,
    w_key,
    w_value,
    offset_bias,
    w_out,
):
    tokens, model = latent.shape
    cols = w_shift.shape[1]
    width = w_query.shape[1]
    heads = width // HEAD_DIM
    chunks = width // 128 if width % 128 == 0 else 1
    each = width // chunks
    sp_count, tp_count = lax.axis_size("sp"), lax.axis_size("tp")
    halo = HALO * GRID_W

    own_context = shape_of((context.shape[0], cols), BF16)
    mod_inputs = (conditioning, ctx_vector, w_shift, w_scale, w_gate)
    partial = call(
        modulation_kernel,
        shape_of((2 * MOD_ROWS + context.shape[0], cols), BF16),
        scratch=[pltpu.VMEM(a.shape, a.dtype) for a in mod_inputs + (own_context,)]
        + [pltpu.SemaphoreType.DMA((6,))],
        in_specs=[HBM] * 6,
    )(*in_hbm(mod_inputs + (context,)))
    mod_own, ctx_own = total_and_context(partial, "sp")
    mod_pieces = pieces_of(mod_own, "tp")

    lanes = GRID_W - offset_bias.shape[2]
    padded = jnp.pad(offset_bias, ((0, 0), (0, 0), (0, lanes)))
    pairs = jnp.concatenate([padded[:, :-1], padded[:, 1:]], axis=2)
    table = call(
        functools.partial(bias_kernel, heads=heads),
        shape_of((2 * WIN_H - 2, heads * GRID_W, 2 * GRID_W), F32),
    )(pairs)

    kv_shapes = (
        shape_of((tokens, 2 * each), BF16),
        shape_of((halo, 2 * each), BF16),
        shape_of((halo, 2 * each), BF16),
    )
    normed, kv_0, send_a_0, send_b_0, mod, gain, *weights = call(
        functools.partial(norm_kernel, tp_count=tp_count, chunks=chunks),
        (shape_of((tokens, model), BF16),)
        + kv_shapes
        + (shape_of((MOD_ROWS, model), F32), shape_of((8, model), F32))
        + (shape_of((model, 2 * each), BF16),) * chunks,
        scratch=[
            pltpu.VMEM((model,), BF16),
            pltpu.VMEM((8, model), F32),
            pltpu.VMEM((8, model), F32),
            pltpu.SemaphoreType.DMA((1 + 2 * chunks,)),
        ],
        in_specs=[VMEM] + [HBM] * 3 + [VMEM] * tp_count,
    )(latent, *in_hbm((norm_gain, w_key, w_value)), *mod_pieces)

    keys_values = [(kv_0, send_a_0, send_b_0)] + [
        call(chunk_kernel, kv_shapes)(normed, weight) for weight in weights[1:]
    ]
    halos = [(pairwise(a, "sp", 0), pairwise(b, "sp", 1)) for _, a, b in keys_values]

    query, resid = call(
        query_kernel, (shape_of((tokens, width), BF16), shape_of((tokens, cols), BF16))
    )(normed, w_query, latent)

    ctx_pieces = pieces_by_bits(ctx_own, "tp")
    ctx_rows = ctx_own.shape[0]
    ctx_all = call(
        functools.partial(context_kernel, masks=[m for m, _ in ctx_pieces], chunks=chunks),
        (shape_of((ctx_rows, 2 * each), BF16),) * chunks,
        scratch=[pltpu.VMEM((ctx_rows, model), BF16)],
    )(mod, gain, *[p for _, p in ctx_pieces], *weights)

    gathered = []
    for c in range(chunks):
        attended = call(
            functools.partial(attention_kernel, chunk=c, sp_count=sp_count),
            shape_of((tokens, each), BF16),
            scratch=[pltpu.VMEM((tokens + 2 * halo, 2 * each), BF16)],
        )(query, keys_values[c][0], *halos[c], table, ctx_all[c])
        found = pieces_by_bits(attended, "tp")
        masks = [mask for mask, _ in found]
        gathered += [piece for _, piece in found]

    return call(
        functools.partial(output_kernel, masks=masks, chunks=chunks),
        shape_of((tokens, cols), BF16),
    )(resid, mod_own, w_out, *gathered)


def solution(mesh):
    return jax.shard_map(
        local,
        mesh=mesh,
        in_specs=(
            P(("grp", "sp"), None),
            P(("grp", "sp")),
            P(("grp", "sp"), None),
            P("sp"),
            P("sp", "tp"),
            P("sp", "tp"),
            P("sp", "tp"),
            P(),
            P(None, "tp"),
            P(None, "tp"),
            P(None, "tp"),
            P("tp", None, None),
            P(None, "tp"),
        ),
        out_specs=P(("grp", "sp"), "tp"),
        check_vma=False,
    )
```

```python
import functools

import jax
import jax.numpy as jnp
from jax import lax
from jax.experimental import pallas as pl
from jax.experimental.pallas import tpu as pltpu
from jax.sharding import PartitionSpec as P

HEAD_DIM = 64
GRID_W = 64
WIN_H = 8
WIN_W = 16
EPSILON = 1e-06
HALO = WIN_H // 2
MASKED = -1e30
SHIFT, CTX_SHIFT, SCALE, CTX_SCALE, GATE, MOD_ROWS = 0, 1, 2, 3, 4, 8

HBM = pl.BlockSpec(memory_space=pltpu.HBM)
VMEM = pl.BlockSpec(memory_space=pltpu.VMEM)
F32 = jnp.float32
BF16 = jnp.bfloat16


def call(kernel, out_shape, scratch=(), vmem_mib=24, **kwargs):
    return pl.pallas_call(
        kernel,
        out_shape=out_shape,
        scratch_shapes=list(scratch),
        compiler_params=pltpu.CompilerParams(vmem_limit_bytes=vmem_mib * 2**20),
        **kwargs,
    )


def in_hbm(arrays):
    return [pltpu.with_memory_space_constraint(a, pltpu.HBM) for a in arrays]


def shape_of(shape, dtype):
    return jax.ShapeDtypeStruct(shape, dtype)


def digits(count):
    unit, found = 1, []
    while unit < count:
        radix = 4 if count // unit % 4 == 0 else 2
        found.append((unit, radix))
        unit *= radix
    return found


def peer(block, axis, mask):
    count = lax.axis_size(axis)
    return lax.ppermute(block, axis, [(i, i ^ mask) for i in range(count)])


def joined(parts):
    sums = None
    for part in parts:
        rows = part[:MOD_ROWS].astype(F32) + part[MOD_ROWS : 2 * MOD_ROWS].astype(F32)
        sums = rows if sums is None else sums + rows
    return sums, jnp.concatenate([part[2 * MOD_ROWS :] for part in parts], axis=0)


def total_and_context(block, axis):
    steps = digits(lax.axis_size(axis))
    for i, (unit, radix) in enumerate(steps):
        far_first = [peer(block, axis, unit * k) for k in reversed(range(1, radix))]
        sums, context = joined([block] + far_first)
        if i + 1 < len(steps):
            high = lax.reduce_precision(sums, 8, 7)
            block = jnp.concatenate([high, sums - high], axis=0).astype(BF16)
            block = jnp.concatenate([block, context], axis=0)
    return sums, context


def pieces_of(block, axis):
    pieces = [block]
    for unit, radix in digits(lax.axis_size(axis)):
        pieces = pieces + [peer(p, axis, unit * k) for k in range(1, radix) for p in pieces]
    return pieces


def pieces_by_bits(block, axis):
    pieces = [(0, block)]
    bit = lax.axis_size(axis) // 2
    while bit:
        pieces = pieces + [(mask ^ bit, peer(p, axis, bit)) for mask, p in pieces]
        bit //= 2
    return pieces


def pairwise(block, axis, first):
    count = lax.axis_size(axis)
    pairs = []
    for low in range(first, count - 1, 2):
        pairs += [(low, low + 1), (low + 1, low)]
    return lax.ppermute(block, axis, pairs)


def silu(v):
    return v / (1.0 + jnp.exp(-v))


def fetch(pairs, sems):
    copies = [
        pltpu.make_async_copy(source, target, sems.at[i]) for i, (source, target) in enumerate(pairs)
    ]
    for copy in copies:
        copy.start()
    return copies


def modulation_kernel(
    cond_hbm, ctx_hbm, w_shift_hbm, w_scale_hbm, w_gate_hbm, context_hbm, out_ref, *scratch
):
    cond_ref, ctx_ref, w_shift_ref, w_scale_ref, w_gate_ref, context_ref, sems = scratch
    cols = w_shift_ref.shape[1]
    own = pl.ds(pl.multiple_of(lax.axis_index("tp") * cols, 128), cols)
    sources = (cond_hbm, ctx_hbm, w_shift_hbm, w_scale_hbm, w_gate_hbm, context_hbm.at[:, own])
    copies = fetch(list(zip(sources, scratch[:-1])), sems)
    copies[0].wait()
    copies[1].wait()
    cond = silu(cond_ref[...].astype(F32)).reshape(1, -1)
    ctx = silu(ctx_ref[...].astype(F32)).reshape(1, -1)
    row = lax.broadcasted_iota(jnp.int32, (MOD_ROWS, cond.shape[1]), 0)
    acts = jnp.where(row % 2 == 0, cond, ctx).astype(BF16)
    copies[2].wait()
    shifts = jnp.dot(acts, w_shift_ref[...], preferred_element_type=F32)
    copies[3].wait()
    scales = jnp.dot(acts, w_scale_ref[...], preferred_element_type=F32)
    copies[4].wait()
    gates = jnp.dot(acts, w_gate_ref[...], preferred_element_type=F32)
    out_row = lax.broadcasted_iota(jnp.int32, shifts.shape, 0)
    sums = jnp.where(out_row < SCALE, shifts, jnp.where(out_row < GATE, scales, gates))
    high = sums.astype(BF16).astype(F32)
    out_ref[: 2 * MOD_ROWS, :] = jnp.concatenate([high, sums - high], axis=0).astype(BF16)
    copies[5].wait()
    out_ref[2 * MOD_ROWS :, :] = context_ref[...]


def bias_table(vectors_ref, out_ref):
    lanes = out_ref.shape[1]
    key = lax.broadcasted_iota(jnp.int32, (GRID_W, lanes), 0)
    query = lax.broadcasted_iota(jnp.int32, (GRID_W, lanes), 1) % GRID_W
    first = jnp.clip(query - WIN_W // 2, 0, GRID_W - WIN_W)
    inside = (key >= first) & (key < first + WIN_W)
    for r in range(2 * WIN_H - 1):
        table = pltpu.roll(
            jnp.broadcast_to(vectors_ref[r : r + 1, :], (GRID_W, lanes)),
            lanes - (WIN_W - 1),
            1,
            stride=1,
            stride_axis=0,
        )
        out_ref[r * GRID_W : (r + 1) * GRID_W, :] = jnp.where(inside, table, MASKED)


def bias_kernel(*refs):
    half = len(refs) // 2
    for vectors_ref, out_ref in zip(refs[:half], refs[half:]):
        bias_table(vectors_ref, out_ref)


def inverse_rms(floats):
    return lax.rsqrt(jnp.mean(floats * floats, axis=-1, keepdims=True) + EPSILON)


def send_halo(kv_ref, send_a_ref, send_b_ref):
    halo = HALO * GRID_W
    last = kv_ref.shape[0] - halo
    odd = lax.axis_index("sp") % 2
    send_a_ref[...] = kv_ref[pl.ds(pl.multiple_of((1 - odd) * last, GRID_W), halo), :]
    send_b_ref[...] = kv_ref[pl.ds(pl.multiple_of(odd * last, GRID_W), halo), :]


def norm_kernel(*refs, tp_count, chunks):
    latent_ref, gain_hbm, wk_hbm, wv_hbm = refs[:4]
    piece_refs = refs[4 : 4 + tp_count]
    outs = refs[4 + tp_count : -4]
    normed_ref, kv_ref, send_a_ref, send_b_ref, mod_ref, gain_out_ref = outs[:6]
    weight_refs = outs[6:]
    gain_ref, factor_ref, offset_ref, sems = refs[-4:]
    tokens, _ = latent_ref.shape
    cols = piece_refs[0].shape[1]
    each = weight_refs[0].shape[1] // 2
    pairs = [(gain_hbm, gain_ref)]
    for c, weight in enumerate(weight_refs):
        at = pl.ds(c * each, each)
        pairs += [(wk_hbm.at[:, at], weight.at[:, :each]), (wv_hbm.at[:, at], weight.at[:, each:])]
    copies = fetch(pairs, sems)
    tp_index = lax.axis_index("tp")
    for k, piece in enumerate(piece_refs):
        offset = pl.multiple_of((tp_index ^ k) * cols, 128)
        mod_ref[:, pl.ds(offset, cols)] = piece[...]
    copies[0].wait()
    gain = gain_ref[...].astype(F32).reshape(1, -1)
    gain_out_ref[...] = jnp.broadcast_to(gain, gain_out_ref.shape)
    factor_ref[...] = jnp.broadcast_to(gain * (1.0 + mod_ref[SCALE : SCALE + 1, :]), factor_ref.shape)
    offset_ref[...] = jnp.broadcast_to(mod_ref[SHIFT : SHIFT + 1, :], offset_ref.shape)
    step = 16

    def body(i, carry):
        at = pl.ds(pl.multiple_of(i * step, step), step)
        floats = latent_ref[at, :].astype(F32)
        scaled = (floats * inverse_rms(floats)).reshape(step // 8, 8, -1)
        result = scaled * factor_ref[...][None] + offset_ref[...][None]
        normed_ref[at, :] = result.reshape(step, -1).astype(BF16)
        return carry

    lax.fori_loop(0, tokens // step, body, 0, unroll=2)
    copies[1].wait()
    copies[2].wait()
    kv_ref[...] = jnp.dot(
        normed_ref[...], weight_refs[0][...], preferred_element_type=F32
    ).astype(BF16)
    send_halo(kv_ref, send_a_ref, send_b_ref)
    for copy in copies[3:]:
        copy.wait()


def chunk_kernel(normed_ref, weight_ref, kv_ref, send_a_ref, send_b_ref):
    kv_ref[...] = jnp.dot(
        normed_ref[...], weight_ref[...], preferred_element_type=F32
    ).astype(BF16)
    send_halo(kv_ref, send_a_ref, send_b_ref)


def query_kernel(normed_ref, wq_ref, latent_ref, q_ref, resid_ref):
    cols = resid_ref.shape[1]
    query = jnp.dot(normed_ref[...], wq_ref[...], preferred_element_type=F32).astype(BF16)
    q_ref[...] = query * BF16(HEAD_DIM**-0.5)
    own = pl.ds(pl.multiple_of(lax.axis_index("tp") * cols, 128), cols)
    resid_ref[...] = latent_ref[:, own]


def context_kernel(*refs, masks, chunks):
    mod_ref, gain_ref = refs[:2]
    piece_refs = refs[2 : 2 + len(masks)]
    weight_refs = refs[2 + len(masks) : 2 + len(masks) + chunks]
    out_refs, whole_ref = refs[2 + len(masks) + chunks : -1], refs[-1]
    cols = piece_refs[0].shape[1]
    tp_index = lax.axis_index("tp")
    for mask, piece in zip(masks, piece_refs):
        whole_ref[:, pl.ds(pl.multiple_of((tp_index ^ mask) * cols, 128), cols)] = piece[...]
    floats = whole_ref[...].astype(F32)
    factor = gain_ref[0:1, :] * (1.0 + mod_ref[CTX_SCALE : CTX_SCALE + 1, :])
    shift = mod_ref[CTX_SHIFT : CTX_SHIFT + 1, :]
    normed = (floats * inverse_rms(floats) * factor + shift).astype(BF16)
    for weight, out in zip(weight_refs, out_refs):
        out[...] = jnp.dot(normed, weight[...], preferred_element_type=F32).astype(BF16)


def attention_kernel(
    q_ref,
    kv_ref,
    recv_a_ref,
    recv_b_ref,
    table_ref,
    ctx_ref,
    out_ref,
    pad_ref,
    score_ref,
    weight_ref,
    *,
    chunk,
    sp_count,
):
    tokens, width = out_ref.shape
    heads = width // HEAD_DIM
    rows = tokens // GRID_W
    halo = HALO * GRID_W
    groups, keys, _ = score_ref.shape
    group = rows // groups
    ctx_rows = ctx_ref.shape[0]
    span = keys - ctx_rows
    sp_index = lax.axis_index("sp")
    odd = sp_index % 2
    far = halo + tokens
    pad_ref[pl.ds(pl.multiple_of((1 - odd) * far, GRID_W), halo), : 2 * width] = recv_a_ref[...]
    pad_ref[pl.ds(pl.multiple_of(odd * far, GRID_W), halo), : 2 * width] = recv_b_ref[...]
    pad_ref[halo : halo + tokens, : 2 * width] = kv_ref[...]
    pad_ref[:, 2 * width :] = jnp.ones((tokens + 2 * halo, width), BF16)
    lane_head = lax.broadcasted_iota(jnp.int32, (1, width), 1) // HEAD_DIM
    picks = [(lane_head == h) for h in range(heads)]
    nt = (((1,), (1,)), ((), ()))
    tn = (((0,), (0,)), ((), ()))

    def start_of(l):
        grid_row = sp_index * rows + l
        first = jnp.clip(grid_row - HALO, 0, sp_count * rows - WIN_H)
        return first - sp_index * rows + HALO, first - grid_row + WIN_H - 1

    def window_of(g):
        return pl.ds(pl.multiple_of(start_of(g * group)[0] * GRID_W, GRID_W), span)

    def score(g):
        left = []
        for l in range(g * group, (g + 1) * group):
            query = q_ref[l * GRID_W : (l + 1) * GRID_W, chunk * width : (chunk + 1) * width]
            left += [jnp.where(pick, query, BF16(0)) for pick in picks]
        left = jnp.concatenate(left, axis=0)
        score_ref[g, :span, :] = lax.dot_general(
            pad_ref[window_of(g), :width], left, nt, preferred_element_type=F32
        )
        score_ref[g, span:, :] = lax.dot_general(
            ctx_ref[:, :width], left, nt, preferred_element_type=F32
        )

    def weigh(g):
        for k in range(group):
            start, offset = start_of(g * group + k)
            shift = start - start_of(g * group)[0]
            lanes = slice(k * width, (k + 1) * width)
            highest = jnp.max(score_ref[g, span:, lanes], axis=0, keepdims=True)
            blocks = []
            for u in range(span // GRID_W):
                row = jnp.clip(u - shift, 0, WIN_H - 1) + offset
                block = table_ref[pl.ds(pl.multiple_of(row * GRID_W, GRID_W), GRID_W), :]
                if u < k or u >= WIN_H:
                    block = jnp.where((u >= shift) & (u < shift + WIN_H), block, MASKED)
                block = block + score_ref[g, u * GRID_W : (u + 1) * GRID_W, lanes]
                blocks.append(block)
                highest = jnp.maximum(highest, jnp.max(block, axis=0, keepdims=True))
            for u, block in enumerate(blocks):
                weight_ref[g, u * GRID_W : (u + 1) * GRID_W, lanes] = jnp.exp(
                    block - highest
                ).astype(BF16)
            weight_ref[g, span:, lanes] = jnp.exp(score_ref[g, span:, lanes] - highest).astype(BF16)

    def mix(g):
        ctx_values = jnp.concatenate(
            [ctx_ref[:, width:], jnp.ones((ctx_rows, width), BF16)], axis=1
        )
        mixed = lax.dot_general(
            weight_ref[g, :span, :],
            pad_ref[window_of(g), width:],
            tn,
            preferred_element_type=F32,
        ) + lax.dot_general(weight_ref[g, span:, :], ctx_values, tn, preferred_element_type=F32)
        mixed = mixed[:, :width] / mixed[:, width:]
        for k in range(group):
            low = k * heads * GRID_W
            result = mixed[low : low + GRID_W]
            for h in range(1, heads):
                low += GRID_W
                result = jnp.where(picks[h], mixed[low : low + GRID_W], result)
            l = g * group + k
            out_ref[l * GRID_W : (l + 1) * GRID_W, :] = result.astype(BF16)

    for g in range(groups):
        score(g)
    for g in range(groups):
        weigh(g)
        if g > 0:
            mix(g - 1)
    mix(groups - 1)


def output_kernel(*refs, masks, chunks):
    resid_ref, mod_ref, w_out_ref = refs[:3]
    piece_refs, out_ref = refs[3:-1], refs[-1]
    tp_index = lax.axis_index("tp")
    count = len(masks)
    width = chunks * piece_refs[0].shape[1]
    branch = None
    for i, mask in enumerate(masks):
        offset = pl.multiple_of((tp_index ^ mask) * width, 128)
        piece = jnp.concatenate([piece_refs[c * count + i][...] for c in range(chunks)], axis=1)
        part = jnp.dot(piece, w_out_ref[pl.ds(offset, width), :], preferred_element_type=F32)
        branch = part if branch is None else branch + part
    out_ref[...] = (resid_ref[...].astype(F32) + mod_ref[GATE : GATE + 1, :] * branch).astype(BF16)


def local(
    latent,
    conditioning,
    context,
    ctx_vector,
    w_shift,
    w_scale,
    w_gate,
    norm_gain,
    w_query,
    w_key,
    w_value,
    offset_bias,
    w_out,
):
    tokens, model = latent.shape
    cols = w_shift.shape[1]
    width = w_query.shape[1]
    heads = width // HEAD_DIM
    chunks = width // 128 if width % 128 == 0 else 1
    each = width // chunks
    sp_count, tp_count = lax.axis_size("sp"), lax.axis_size("tp")
    halo = HALO * GRID_W

    own_context = shape_of((context.shape[0], cols), BF16)
    mod_inputs = (conditioning, ctx_vector, w_shift, w_scale, w_gate)
    partial = call(
        modulation_kernel,
        shape_of((2 * MOD_ROWS + context.shape[0], cols), BF16),
        scratch=[pltpu.VMEM(a.shape, a.dtype) for a in mod_inputs + (own_context,)]
        + [pltpu.SemaphoreType.DMA((6,))],
        in_specs=[HBM] * 6,
    )(*in_hbm(mod_inputs + (context,)))
    mod_own, ctx_own = total_and_context(partial, "sp")
    mod_pieces = pieces_of(mod_own, "tp")

    fill = GRID_W - offset_bias.shape[2]
    flipped = jnp.pad(offset_bias[:, :, ::-1], ((0, 0), (0, 0), (0, fill)))
    vectors = [
        jnp.concatenate(list(flipped[c * heads // chunks : (c + 1) * heads // chunks]), axis=1)
        for c in range(chunks)
    ]
    table_shape = shape_of(((2 * WIN_H - 1) * GRID_W, each), F32)
    tables = call(bias_kernel, (table_shape,) * chunks)(*vectors)

    kv_shapes = (
        shape_of((tokens, 2 * each), BF16),
        shape_of((halo, 2 * each), BF16),
        shape_of((halo, 2 * each), BF16),
    )
    normed, kv_0, send_a_0, send_b_0, mod, gain, *weights = call(
        functools.partial(norm_kernel, tp_count=tp_count, chunks=chunks),
        (shape_of((tokens, model), BF16),)
        + kv_shapes
        + (shape_of((MOD_ROWS, model), F32), shape_of((8, model), F32))
        + (shape_of((model, 2 * each), BF16),) * chunks,
        scratch=[
            pltpu.VMEM((model,), BF16),
            pltpu.VMEM((8, model), F32),
            pltpu.VMEM((8, model), F32),
            pltpu.SemaphoreType.DMA((1 + 2 * chunks,)),
        ],
        in_specs=[VMEM] + [HBM] * 3 + [VMEM] * tp_count,
    )(latent, *in_hbm((norm_gain, w_key, w_value)), *mod_pieces)

    keys_values = [(kv_0, send_a_0, send_b_0)] + [
        call(chunk_kernel, kv_shapes)(normed, weight) for weight in weights[1:]
    ]
    halos = [(pairwise(a, "sp", 0), pairwise(b, "sp", 1)) for _, a, b in keys_values]

    query, resid = call(
        query_kernel, (shape_of((tokens, width), BF16), shape_of((tokens, cols), BF16))
    )(normed, w_query, latent)

    ctx_pieces = pieces_by_bits(ctx_own, "tp")
    ctx_rows = ctx_own.shape[0]
    ctx_all = call(
        functools.partial(context_kernel, masks=[m for m, _ in ctx_pieces], chunks=chunks),
        (shape_of((ctx_rows, 2 * each), BF16),) * chunks,
        scratch=[pltpu.VMEM((ctx_rows, model), BF16)],
    )(mod, gain, *[p for _, p in ctx_pieces], *weights)

    rows = tokens // GRID_W
    group = 2 if rows % 2 == 0 else 1
    keys = (WIN_H + group - 1) * GRID_W + ctx_rows
    gathered = []
    for c in range(chunks):
        attended = call(
            functools.partial(attention_kernel, chunk=c, sp_count=sp_count),
            shape_of((tokens, each), BF16),
            scratch=[
                pltpu.VMEM((tokens + 2 * halo, 3 * each), BF16),
                pltpu.VMEM((rows // group, keys, group * each), F32),
                pltpu.VMEM((rows // group, keys, group * each), BF16),
            ],
        )(query, keys_values[c][0], *halos[c], tables[c], ctx_all[c])
        found = pieces_by_bits(attended, "tp")
        masks = [mask for mask, _ in found]
        gathered += [piece for _, piece in found]

    return call(
        functools.partial(output_kernel, masks=masks, chunks=chunks),
        shape_of((tokens, cols), BF16),
    )(resid, mod_own, w_out, *gathered)


def solution(mesh):
    return jax.shard_map(
        local,
        mesh=mesh,
        in_specs=(
            P(("grp", "sp"), None),
            P(("grp", "sp")),
            P(("grp", "sp"), None),
            P("sp"),
            P("sp", "tp"),
            P("sp", "tp"),
            P("sp", "tp"),
            P(),
            P(None, "tp"),
            P(None, "tp"),
            P(None, "tp"),
            P("tp", None, None),
            P(None, "tp"),
        ),
        out_specs=P(("grp", "sp"), "tp"),
        check_vma=False,
    )
```

```python
import functools

import jax
import jax.numpy as jnp
from jax import lax
from jax.experimental import pallas as pl
from jax.experimental.pallas import tpu as pltpu
from jax.sharding import PartitionSpec as P


HEAD_DIM = 64
GRID_W = 64
WIN_H = 8
WIN_W = 16
EPSILON = 1e-06
HALO = WIN_H // 2
MASKED = -1e30
SHIFT, CTX_SHIFT, SCALE, CTX_SCALE, GATE, MOD_ROWS = 0, 1, 2, 3, 4, 8

HBM = pl.BlockSpec(memory_space=pltpu.HBM)
VMEM = pl.BlockSpec(memory_space=pltpu.VMEM)
F32 = jnp.float32
BF16 = jnp.bfloat16


def call(kernel, out_shape, scratch=(), vmem_mib=24, **kwargs):
    return pl.pallas_call(
        kernel,
        out_shape=out_shape,
        scratch_shapes=list(scratch),
        compiler_params=pltpu.CompilerParams(vmem_limit_bytes=vmem_mib * 2**20),
        **kwargs,
    )


def in_hbm(arrays):
    return [pltpu.with_memory_space_constraint(a, pltpu.HBM) for a in arrays]


def shape_of(shape, dtype):
    return jax.ShapeDtypeStruct(shape, dtype)


def digits(count):
    unit, found = 1, []
    while unit < count:
        radix = 4 if count // unit % 4 == 0 else 2
        found.append((unit, radix))
        unit *= radix
    return found


def peer(block, axis, mask):
    count = lax.axis_size(axis)
    return lax.ppermute(block, axis, [(i, i ^ mask) for i in range(count)])


def joined(parts):
    sums = None
    for part in parts:
        rows = part[:MOD_ROWS].astype(F32) + part[MOD_ROWS : 2 * MOD_ROWS].astype(F32)
        sums = rows if sums is None else sums + rows
    return sums, jnp.concatenate([part[2 * MOD_ROWS :] for part in parts], axis=0)


def total_and_context(block, axis):
    steps = digits(lax.axis_size(axis))
    for i, (unit, radix) in enumerate(steps):
        far_first = [peer(block, axis, unit * k) for k in reversed(range(1, radix))]
        sums, context = joined([block] + far_first)
        if i + 1 < len(steps):
            high = lax.reduce_precision(sums, 8, 7)
            block = jnp.concatenate([high, sums - high], axis=0).astype(BF16)
            block = jnp.concatenate([block, context], axis=0)
    return sums, context


def pieces_of(block, axis):
    pieces = [block]
    for unit, radix in digits(lax.axis_size(axis)):
        pieces = pieces + [peer(p, axis, unit * k) for k in range(1, radix) for p in pieces]
    return pieces


def pieces_by_bits(block, axis):
    pieces = [(0, block)]
    bit = lax.axis_size(axis) // 2
    while bit:
        pieces = pieces + [(mask ^ bit, peer(p, axis, bit)) for mask, p in pieces]
        bit //= 2
    return pieces


def pairwise(block, axis, first):
    count = lax.axis_size(axis)
    pairs = []
    for low in range(first, count - 1, 2):
        pairs += [(low, low + 1), (low + 1, low)]
    return lax.ppermute(block, axis, pairs)


def silu(v):
    return v / (1.0 + jnp.exp(-v))


def fetch(pairs, sems):
    copies = [
        pltpu.make_async_copy(source, target, sems.at[i]) for i, (source, target) in enumerate(pairs)
    ]
    for copy in copies:
        copy.start()
    return copies


def modulation_kernel(
    cond_hbm, ctx_hbm, w_shift_hbm, w_scale_hbm, w_gate_hbm, context_hbm, out_ref, *scratch
):
    cond_ref, ctx_ref, w_shift_ref, w_scale_ref, w_gate_ref, context_ref, sems = scratch
    cols = w_shift_ref.shape[1]
    own = pl.ds(pl.multiple_of(lax.axis_index("tp") * cols, 128), cols)
    sources = (cond_hbm, ctx_hbm, w_shift_hbm, w_scale_hbm, w_gate_hbm, context_hbm.at[:, own])
    copies = fetch(list(zip(sources, scratch[:-1])), sems)
    copies[0].wait()
    copies[1].wait()
    cond = silu(cond_ref[...].astype(F32)).reshape(1, -1)
    ctx = silu(ctx_ref[...].astype(F32)).reshape(1, -1)
    row = lax.broadcasted_iota(jnp.int32, (MOD_ROWS, cond.shape[1]), 0)
    acts = jnp.where(row % 2 == 0, cond, ctx).astype(BF16)
    copies[2].wait()
    shifts = jnp.dot(acts, w_shift_ref[...], preferred_element_type=F32)
    copies[3].wait()
    scales = jnp.dot(acts, w_scale_ref[...], preferred_element_type=F32)
    copies[4].wait()
    gates = jnp.dot(acts, w_gate_ref[...], preferred_element_type=F32)
    out_row = lax.broadcasted_iota(jnp.int32, shifts.shape, 0)
    sums = jnp.where(out_row < SCALE, shifts, jnp.where(out_row < GATE, scales, gates))
    high = sums.astype(BF16).astype(F32)
    out_ref[: 2 * MOD_ROWS, :] = jnp.concatenate([high, sums - high], axis=0).astype(BF16)
    copies[5].wait()
    out_ref[2 * MOD_ROWS :, :] = context_ref[...]


def bias_table(vectors_ref, out_ref):
    lanes = out_ref.shape[1]
    key = lax.broadcasted_iota(jnp.int32, (GRID_W, lanes), 0)
    query = lax.broadcasted_iota(jnp.int32, (GRID_W, lanes), 1) % GRID_W
    first = jnp.clip(query - WIN_W // 2, 0, GRID_W - WIN_W)
    inside = (key >= first) & (key < first + WIN_W)
    for r in range(2 * WIN_H - 1):
        table = pltpu.roll(
            jnp.broadcast_to(vectors_ref[r : r + 1, :], (GRID_W, lanes)),
            lanes - (WIN_W - 1),
            1,
            stride=1,
            stride_axis=0,
        )
        out_ref[r * GRID_W : (r + 1) * GRID_W, :] = jnp.where(inside, table, MASKED)


def inverse_rms(floats):
    return lax.rsqrt(jnp.mean(floats * floats, axis=-1, keepdims=True) + EPSILON)


def send_halo(kv_ref, send_a_ref, send_b_ref):
    halo = HALO * GRID_W
    last = kv_ref.shape[0] - halo
    odd = lax.axis_index("sp") % 2
    send_a_ref[...] = kv_ref[pl.ds(pl.multiple_of((1 - odd) * last, GRID_W), halo), :]
    send_b_ref[...] = kv_ref[pl.ds(pl.multiple_of(odd * last, GRID_W), halo), :]


def prepare_kernel(*refs, chunks):
    latent_ref, gain_hbm, wk_hbm, wv_hbm = refs[:4]
    vector_refs = refs[4 : 4 + chunks]
    inverse_ref, gain_out_ref = refs[4 + chunks : 6 + chunks]
    weight_refs = refs[6 + chunks : 6 + 2 * chunks]
    table_refs = refs[6 + 2 * chunks : -2]
    gain_ref, sems = refs[-2:]
    tokens, _ = latent_ref.shape
    each = weight_refs[0].shape[1] // 2
    pairs = [(gain_hbm, gain_ref)]
    for c, weight in enumerate(weight_refs):
        at = pl.ds(c * each, each)
        pairs += [(wk_hbm.at[:, at], weight.at[:, :each]), (wv_hbm.at[:, at], weight.at[:, each:])]
    copies = fetch(pairs, sems)
    for vectors_ref, table_ref in zip(vector_refs, table_refs):
        bias_table(vectors_ref, table_ref)
    step = 16

    def body(i, carry):
        at = pl.ds(pl.multiple_of(i * step, step), step)
        inverse = inverse_rms(latent_ref[at, :].astype(F32))
        inverse_ref[at, :] = jnp.broadcast_to(inverse, (step, 128))
        return carry

    lax.fori_loop(0, tokens // step, body, 0, unroll=2)
    copies[0].wait()
    gain = gain_ref[...].astype(F32).reshape(1, -1)
    gain_out_ref[...] = jnp.broadcast_to(gain, gain_out_ref.shape)
    for copy in copies[1:]:
        copy.wait()


def norm_kernel(*refs):
    latent_ref, inverse_ref, gain_ref, weight_ref = refs[:4]
    piece_refs = refs[4:-7]
    normed_ref, kv_ref, send_a_ref, send_b_ref, mod_ref, factor_ref, offset_ref = refs[-7:]
    tokens, model = latent_ref.shape
    cols = piece_refs[0].shape[1]
    tp_index = lax.axis_index("tp")
    for k, piece in enumerate(piece_refs):
        offset = pl.multiple_of((tp_index ^ k) * cols, 128)
        mod_ref[:, pl.ds(offset, cols)] = piece[...]
    factor_ref[...] = gain_ref[...] * (1.0 + mod_ref[SCALE : SCALE + 1, :])
    offset_ref[...] = jnp.broadcast_to(mod_ref[SHIFT : SHIFT + 1, :], offset_ref.shape)
    step = 16

    def body(i, carry):
        at = pl.ds(pl.multiple_of(i * step, step), step)
        inverse = inverse_ref[at, :].reshape(step // 8, 8, 128)
        for j in range(0, model, 128):
            lanes = slice(j, j + 128)
            floats = latent_ref[at, lanes].astype(F32).reshape(step // 8, 8, 128)
            result = floats * inverse * factor_ref[:, lanes][None] + offset_ref[:, lanes][None]
            normed_ref[at, lanes] = result.reshape(step, 128).astype(BF16)
        return carry

    lax.fori_loop(0, tokens // step, body, 0, unroll=4)
    kv_ref[...] = jnp.dot(
        normed_ref[...], weight_ref[...], preferred_element_type=F32
    ).astype(BF16)
    send_halo(kv_ref, send_a_ref, send_b_ref)


def chunk_kernel(normed_ref, weight_ref, kv_ref, send_a_ref, send_b_ref):
    kv_ref[...] = jnp.dot(
        normed_ref[...], weight_ref[...], preferred_element_type=F32
    ).astype(BF16)
    send_halo(kv_ref, send_a_ref, send_b_ref)


def query_kernel(normed_ref, wq_ref, latent_ref, q_ref, resid_ref):
    cols = resid_ref.shape[1]
    query = jnp.dot(normed_ref[...], wq_ref[...], preferred_element_type=F32).astype(BF16)
    q_ref[...] = query * BF16(HEAD_DIM**-0.5)
    own = pl.ds(pl.multiple_of(lax.axis_index("tp") * cols, 128), cols)
    resid_ref[...] = latent_ref[:, own]


def context_kernel(*refs, masks, chunks):
    mod_ref, gain_ref = refs[:2]
    piece_refs = refs[2 : 2 + len(masks)]
    weight_refs = refs[2 + len(masks) : 2 + len(masks) + chunks]
    out_refs, whole_ref = refs[2 + len(masks) + chunks : -1], refs[-1]
    cols = piece_refs[0].shape[1]
    tp_index = lax.axis_index("tp")
    for mask, piece in zip(masks, piece_refs):
        whole_ref[:, pl.ds(pl.multiple_of((tp_index ^ mask) * cols, 128), cols)] = piece[...]
    floats = whole_ref[...].astype(F32)
    factor = gain_ref[0:1, :] * (1.0 + mod_ref[CTX_SCALE : CTX_SCALE + 1, :])
    shift = mod_ref[CTX_SHIFT : CTX_SHIFT + 1, :]
    normed = (floats * inverse_rms(floats) * factor + shift).astype(BF16)
    for weight, out in zip(weight_refs, out_refs):
        out[...] = jnp.dot(normed, weight[...], preferred_element_type=F32).astype(BF16)


def attention_kernel(
    q_ref,
    kv_ref,
    recv_a_ref,
    recv_b_ref,
    table_ref,
    ctx_ref,
    out_ref,
    pad_ref,
    score_ref,
    weight_ref,
    *,
    chunk,
    sp_count,
):
    tokens, width = out_ref.shape
    heads = width // HEAD_DIM
    rows = tokens // GRID_W
    halo = HALO * GRID_W
    groups, keys, _ = score_ref.shape
    group = rows // groups
    ctx_rows = ctx_ref.shape[0]
    span = keys - ctx_rows
    sp_index = lax.axis_index("sp")
    odd = sp_index % 2
    far = halo + tokens
    pad_ref[pl.ds(pl.multiple_of((1 - odd) * far, GRID_W), halo), : 2 * width] = recv_a_ref[...]
    pad_ref[pl.ds(pl.multiple_of(odd * far, GRID_W), halo), : 2 * width] = recv_b_ref[...]
    pad_ref[halo : halo + tokens, : 2 * width] = kv_ref[...]
    pad_ref[:, 2 * width :] = jnp.ones((tokens + 2 * halo, width), BF16)
    lane_head = lax.broadcasted_iota(jnp.int32, (1, width), 1) // HEAD_DIM
    picks = [(lane_head == h) for h in range(heads)]
    nt = (((1,), (1,)), ((), ()))
    tn = (((0,), (0,)), ((), ()))

    def start_of(l):
        grid_row = sp_index * rows + l
        first = jnp.clip(grid_row - HALO, 0, sp_count * rows - WIN_H)
        return first - sp_index * rows + HALO, first - grid_row + WIN_H - 1

    def window_of(g):
        return pl.ds(pl.multiple_of(start_of(g * group)[0] * GRID_W, GRID_W), span)

    def score(g):
        left = []
        for l in range(g * group, (g + 1) * group):
            query = q_ref[l * GRID_W : (l + 1) * GRID_W, chunk * width : (chunk + 1) * width]
            left += [jnp.where(pick, query, BF16(0)) for pick in picks]
        left = jnp.concatenate(left, axis=0)
        score_ref[g, :span, :] = lax.dot_general(
            pad_ref[window_of(g), :width], left, nt, preferred_element_type=F32
        )
        score_ref[g, span:, :] = lax.dot_general(
            ctx_ref[:, :width], left, nt, preferred_element_type=F32
        )

    def weigh(g):
        for k in range(group):
            start, offset = start_of(g * group + k)
            shift = start - start_of(g * group)[0]
            lanes = slice(k * width, (k + 1) * width)
            highest = jnp.max(score_ref[g, span:, lanes], axis=0, keepdims=True)
            blocks = []
            for u in range(span // GRID_W):
                row = jnp.clip(u - shift, 0, WIN_H - 1) + offset
                block = table_ref[pl.ds(pl.multiple_of(row * GRID_W, GRID_W), GRID_W), :]
                if u < k or u >= WIN_H:
                    block = jnp.where((u >= shift) & (u < shift + WIN_H), block, MASKED)
                block = block + score_ref[g, u * GRID_W : (u + 1) * GRID_W, lanes]
                blocks.append(block)
                highest = jnp.maximum(highest, jnp.max(block, axis=0, keepdims=True))
            for u, block in enumerate(blocks):
                weight_ref[g, u * GRID_W : (u + 1) * GRID_W, lanes] = jnp.exp(
                    block - highest
                ).astype(BF16)
            weight_ref[g, span:, lanes] = jnp.exp(score_ref[g, span:, lanes] - highest).astype(BF16)

    def mix(g):
        ctx_values = jnp.concatenate(
            [ctx_ref[:, width:], jnp.ones((ctx_rows, width), BF16)], axis=1
        )
        mixed = lax.dot_general(
            weight_ref[g, :span, :],
            pad_ref[window_of(g), width:],
            tn,
            preferred_element_type=F32,
        ) + lax.dot_general(weight_ref[g, span:, :], ctx_values, tn, preferred_element_type=F32)
        mixed = mixed[:, :width] / mixed[:, width:]
        for k in range(group):
            low = k * heads * GRID_W
            result = mixed[low : low + GRID_W]
            for h in range(1, heads):
                low += GRID_W
                result = jnp.where(picks[h], mixed[low : low + GRID_W], result)
            l = g * group + k
            out_ref[l * GRID_W : (l + 1) * GRID_W, :] = result.astype(BF16)

    for g in range(groups):
        score(g)
    for g in range(groups):
        weigh(g)
        if g > 0:
            mix(g - 1)
    mix(groups - 1)


def output_kernel(*refs, masks, chunk, chunks):
    count = len(masks)
    w_out_ref, piece_refs = refs[0], refs[1 : 1 + count]
    more, out_ref = list(refs[1 + count : -1]), refs[-1]
    tp_index = lax.axis_index("tp")
    each = piece_refs[0].shape[1]
    rows = [
        w_out_ref[pl.ds(pl.multiple_of(((tp_index ^ m) * chunks + chunk) * each, 128), each), :]
        for m in masks
    ]
    branch = jnp.dot(
        jnp.concatenate([piece[...] for piece in piece_refs], axis=1),
        jnp.concatenate(rows, axis=0),
        preferred_element_type=F32,
    )
    if chunk > 0:
        branch = branch + more.pop(0)[...]
    if chunk == chunks - 1:
        resid_ref, mod_ref = more
        branch = resid_ref[...].astype(F32) + mod_ref[GATE : GATE + 1, :] * branch
    out_ref[...] = branch.astype(out_ref.dtype)


def local(
    latent,
    conditioning,
    context,
    ctx_vector,
    w_shift,
    w_scale,
    w_gate,
    norm_gain,
    w_query,
    w_key,
    w_value,
    offset_bias,
    w_out,
):
    tokens, model = latent.shape
    cols = w_shift.shape[1]
    width = w_query.shape[1]
    heads = width // HEAD_DIM
    chunks = width // 128 if width % 128 == 0 else 1
    each = width // chunks
    sp_count = lax.axis_size("sp")
    halo = HALO * GRID_W

    own_context = shape_of((context.shape[0], cols), BF16)
    mod_inputs = (conditioning, ctx_vector, w_shift, w_scale, w_gate)
    partial = call(
        modulation_kernel,
        shape_of((2 * MOD_ROWS + context.shape[0], cols), BF16),
        scratch=[pltpu.VMEM(a.shape, a.dtype) for a in mod_inputs + (own_context,)]
        + [pltpu.SemaphoreType.DMA((6,))],
        in_specs=[HBM] * 6,
    )(*in_hbm(mod_inputs + (context,)))
    mod_own, ctx_own = total_and_context(partial, "sp")
    mod_pieces = pieces_of(mod_own, "tp")

    fill = GRID_W - offset_bias.shape[2]
    flipped = jnp.pad(offset_bias[:, :, ::-1], ((0, 0), (0, 0), (0, fill)))
    vectors = [
        jnp.concatenate(list(flipped[c * heads // chunks : (c + 1) * heads // chunks]), axis=1)
        for c in range(chunks)
    ]
    table_shape = shape_of(((2 * WIN_H - 1) * GRID_W, each), F32)
    inverse, gain, *prepared = call(
        functools.partial(prepare_kernel, chunks=chunks),
        (shape_of((tokens, 128), F32), shape_of((8, model), F32))
        + (shape_of((model, 2 * each), BF16),) * chunks
        + (table_shape,) * chunks,
        scratch=[pltpu.VMEM((model,), BF16), pltpu.SemaphoreType.DMA((1 + 2 * chunks,))],
        in_specs=[VMEM] + [HBM] * 3 + [VMEM] * chunks,
    )(latent, *in_hbm((norm_gain, w_key, w_value)), *vectors)
    weights, tables = prepared[:chunks], prepared[chunks:]

    kv_shapes = (
        shape_of((tokens, 2 * each), BF16),
        shape_of((halo, 2 * each), BF16),
        shape_of((halo, 2 * each), BF16),
    )
    normed, kv_0, send_a_0, send_b_0, mod = call(
        norm_kernel,
        (shape_of((tokens, model), BF16),) + kv_shapes + (shape_of((MOD_ROWS, model), F32),),
        scratch=[pltpu.VMEM((8, model), F32), pltpu.VMEM((8, model), F32)],
    )(latent, inverse, gain, weights[0], *mod_pieces)

    keys_values = [(kv_0, send_a_0, send_b_0)]
    for c in range(1, chunks):
        keys_values.append(call(chunk_kernel, kv_shapes)(normed, weights[c]))
    halos = [
        (pairwise(a, "sp", 0), pairwise(b, "sp", 1))
        for _, a, b in keys_values
    ]

    query, resid = call(
        query_kernel, (shape_of((tokens, width), BF16), shape_of((tokens, cols), BF16))
    )(normed, w_query, latent)

    ctx_pieces = pieces_by_bits(ctx_own, "tp")
    ctx_rows = ctx_own.shape[0]
    ctx_call = call(
        functools.partial(context_kernel, masks=[m for m, _ in ctx_pieces], chunks=chunks),
        (shape_of((ctx_rows, 2 * each), BF16),) * chunks,
        scratch=[pltpu.VMEM((ctx_rows, model), BF16)],
    )
    ctx_all = ctx_call(mod, gain, *[p for _, p in ctx_pieces], *weights)

    rows = tokens // GRID_W
    group = 2 if rows % 2 == 0 else 1
    keys = (WIN_H + group - 1) * GRID_W + ctx_rows
    branch = []
    for c in range(chunks):
        attended = call(
            functools.partial(attention_kernel, chunk=c, sp_count=sp_count),
            shape_of((tokens, each), BF16),
            scratch=[
                pltpu.VMEM((tokens + 2 * halo, 3 * each), BF16),
                pltpu.VMEM((rows // group, keys, group * each), F32),
                pltpu.VMEM((rows // group, keys, group * each), BF16),
            ],
        )(query, keys_values[c][0], *halos[c], tables[c], ctx_all[c])
        found = pieces_by_bits(attended, "tp")
        last = c == chunks - 1
        branch = [
            call(
                functools.partial(
                    output_kernel, masks=[m for m, _ in found], chunk=c, chunks=chunks
                ),
                shape_of((tokens, cols), BF16 if last else F32),
            )(w_out, *[p for _, p in found], *branch, *([resid, mod_own] if last else []))
        ]
    return branch[0]


def solution(mesh):
    return jax.shard_map(
        local,
        mesh=mesh,
        in_specs=(
            P(("grp", "sp"), None),
            P(("grp", "sp")),
            P(("grp", "sp"), None),
            P("sp"),
            P("sp", "tp"),
            P("sp", "tp"),
            P("sp", "tp"),
            P(),
            P(None, "tp"),
            P(None, "tp"),
            P(None, "tp"),
            P("tp", None, None),
            P(None, "tp"),
        ),
        out_specs=P(("grp", "sp"), "tp"),
        check_vma=False,
    )
```

```python
import functools

import jax
import jax.numpy as jnp
from jax import lax
from jax.experimental import pallas as pl
from jax.experimental.pallas import tpu as pltpu
from jax.sharding import PartitionSpec as P


HEAD_DIM = 64
GRID_W = 64
WIN_H = 8
WIN_W = 16
EPSILON = 1e-06
HALO = WIN_H // 2
MASKED = -1e30
LOG2_E = 1.4426950408889634
SHIFT, CTX_SHIFT, SCALE, CTX_SCALE, GATE, MOD_ROWS = 0, 1, 2, 3, 4, 8

HBM = pl.BlockSpec(memory_space=pltpu.HBM)
VMEM = pl.BlockSpec(memory_space=pltpu.VMEM)
F32 = jnp.float32
BF16 = jnp.bfloat16


def call(kernel, out_shape, scratch=(), vmem_mib=24, **kwargs):
    return pl.pallas_call(
        kernel,
        out_shape=out_shape,
        scratch_shapes=list(scratch),
        compiler_params=pltpu.CompilerParams(vmem_limit_bytes=vmem_mib * 2**20),
        **kwargs,
    )


def in_hbm(arrays):
    return [pltpu.with_memory_space_constraint(a, pltpu.HBM) for a in arrays]


def shape_of(shape, dtype):
    return jax.ShapeDtypeStruct(shape, dtype)


def digits(count):
    unit, found = 1, []
    while unit < count:
        radix = 4 if count // unit % 4 == 0 else 2
        found.append((unit, radix))
        unit *= radix
    return found


def peer(block, axis, mask):
    count = lax.axis_size(axis)
    return lax.ppermute(block, axis, [(i, i ^ mask) for i in range(count)])


def joined(parts):
    sums = None
    for part in parts:
        rows = part[:MOD_ROWS].astype(F32) + part[MOD_ROWS : 2 * MOD_ROWS].astype(F32)
        sums = rows if sums is None else sums + rows
    return sums, jnp.concatenate([part[2 * MOD_ROWS :] for part in parts], axis=0)


def total_and_context(block, axis):
    steps = digits(lax.axis_size(axis))
    for i, (unit, radix) in enumerate(steps):
        far_first = [peer(block, axis, unit * k) for k in reversed(range(1, radix))]
        sums, context = joined([block] + far_first)
        if i + 1 < len(steps):
            high = lax.reduce_precision(sums, 8, 7)
            block = jnp.concatenate([high, sums - high], axis=0).astype(BF16)
            block = jnp.concatenate([block, context], axis=0)
    return sums, context


def pieces_of(block, axis):
    pieces = [block]
    for unit, radix in digits(lax.axis_size(axis)):
        pieces = pieces + [peer(p, axis, unit * k) for k in range(1, radix) for p in pieces]
    return pieces


def pieces_by_bits(block, axis):
    pieces = [(0, block)]
    bit = lax.axis_size(axis) // 2
    while bit:
        pieces = pieces + [(mask ^ bit, peer(p, axis, bit)) for mask, p in pieces]
        bit //= 2
    return pieces


def pairwise(block, axis, first):
    count = lax.axis_size(axis)
    pairs = []
    for low in range(first, count - 1, 2):
        pairs += [(low, low + 1), (low + 1, low)]
    return lax.ppermute(block, axis, pairs)


def silu(v):
    return v / (1.0 + jnp.exp(-v))


def fetch(pairs, sems):
    copies = [
        pltpu.make_async_copy(source, target, sems.at[i]) for i, (source, target) in enumerate(pairs)
    ]
    for copy in copies:
        copy.start()
    return copies


def modulation_kernel(
    cond_hbm, ctx_hbm, w_shift_hbm, w_scale_hbm, w_gate_hbm, context_hbm, out_ref, *scratch
):
    cond_ref, ctx_ref, w_shift_ref, w_scale_ref, w_gate_ref, context_ref, sems = scratch
    cols = w_shift_ref.shape[1]
    own = pl.ds(pl.multiple_of(lax.axis_index("tp") * cols, 128), cols)
    sources = (cond_hbm, ctx_hbm, w_shift_hbm, w_scale_hbm, w_gate_hbm, context_hbm.at[:, own])
    copies = fetch(list(zip(sources, scratch[:-1])), sems)
    copies[0].wait()
    copies[1].wait()
    cond = silu(cond_ref[...].astype(F32)).reshape(1, -1)
    ctx = silu(ctx_ref[...].astype(F32)).reshape(1, -1)
    row = lax.broadcasted_iota(jnp.int32, (MOD_ROWS, cond.shape[1]), 0)
    acts = jnp.where(row % 2 == 0, cond, ctx).astype(BF16)
    copies[2].wait()
    shifts = jnp.dot(acts, w_shift_ref[...], preferred_element_type=F32)
    copies[3].wait()
    scales = jnp.dot(acts, w_scale_ref[...], preferred_element_type=F32)
    copies[4].wait()
    gates = jnp.dot(acts, w_gate_ref[...], preferred_element_type=F32)
    out_row = lax.broadcasted_iota(jnp.int32, shifts.shape, 0)
    sums = jnp.where(out_row < SCALE, shifts, jnp.where(out_row < GATE, scales, gates))
    high = sums.astype(BF16).astype(F32)
    out_ref[: 2 * MOD_ROWS, :] = jnp.concatenate([high, sums - high], axis=0).astype(BF16)
    copies[5].wait()
    out_ref[2 * MOD_ROWS :, :] = context_ref[...]


def bias_table(vectors_ref, out_ref):
    lanes = out_ref.shape[1]
    key = lax.broadcasted_iota(jnp.int32, (GRID_W, lanes), 0)
    query = lax.broadcasted_iota(jnp.int32, (GRID_W, lanes), 1) % GRID_W
    first = jnp.clip(query - WIN_W // 2, 0, GRID_W - WIN_W)
    inside = (key >= first) & (key < first + WIN_W)
    for r in range(2 * WIN_H - 1):
        table = pltpu.roll(
            jnp.broadcast_to(vectors_ref[r : r + 1, :], (GRID_W, lanes)),
            lanes - (WIN_W - 1),
            1,
            stride=1,
            stride_axis=0,
        )
        out_ref[r * GRID_W : (r + 1) * GRID_W, :] = jnp.where(inside, table * LOG2_E, MASKED)


def inverse_rms(floats):
    return lax.rsqrt(jnp.mean(floats * floats, axis=-1, keepdims=True) + EPSILON)


def send_halo(kv_refs, send_refs, low_side):
    halo, _ = send_refs[0].shape
    at = pl.ds(pl.multiple_of(low_side * (kv_refs[0].shape[0] - halo), GRID_W), halo)
    each = kv_refs[0].shape[1]
    for c, kv_ref in enumerate(kv_refs):
        if len(send_refs) > 1:
            send_refs[c][...] = kv_ref[at, :]
        else:
            send_refs[0][:, c * each : (c + 1) * each] = kv_ref[at, :]


def prepare_kernel(*refs, chunks):
    latent_ref, gain_hbm, wk_hbm, wv_hbm = refs[:4]
    vector_refs = refs[4 : 4 + chunks]
    inverse_ref, gain_out_ref = refs[4 + chunks : 6 + chunks]
    weight_refs = refs[6 + chunks : 6 + 2 * chunks]
    table_refs = refs[6 + 2 * chunks : -2]
    gain_ref, sems = refs[-2:]
    tokens, _ = latent_ref.shape
    each = weight_refs[0].shape[1] // 2
    pairs = [(gain_hbm, gain_ref)]
    for c, weight in enumerate(weight_refs):
        at = pl.ds(c * each, each)
        pairs += [(wk_hbm.at[:, at], weight.at[:, :each]), (wv_hbm.at[:, at], weight.at[:, each:])]
    copies = fetch(pairs, sems)
    for vectors_ref, table_ref in zip(vector_refs, table_refs):
        bias_table(vectors_ref, table_ref)
    step = 16

    def body(i, carry):
        at = pl.ds(pl.multiple_of(i * step, step), step)
        inverse = inverse_rms(latent_ref[at, :].astype(F32))
        inverse_ref[at, :] = jnp.broadcast_to(inverse, (step, 128))
        return carry

    lax.fori_loop(0, tokens // step, body, 0, unroll=2)
    copies[0].wait()
    gain = gain_ref[...].astype(F32).reshape(1, -1)
    gain_out_ref[...] = jnp.broadcast_to(gain, gain_out_ref.shape)
    for copy in copies[1:]:
        copy.wait()


def norm_kernel(*refs, chunks, tp_count, evens):
    latent_ref, inverse_ref, gain_ref = refs[:3]
    weight_refs, piece_refs = refs[3 : 3 + chunks], refs[3 + chunks : 3 + chunks + tp_count]
    normed_ref, mod_ref = refs[3 + chunks + tp_count : 5 + chunks + tp_count]
    kv_refs = refs[5 + chunks + tp_count : 5 + 2 * chunks + tp_count]
    send_refs = refs[5 + 2 * chunks + tp_count : -2]
    factor_ref, offset_ref = refs[-2:]
    tokens, model = latent_ref.shape
    cols = piece_refs[0].shape[1]
    tp_index = lax.axis_index("tp")
    for k, piece in enumerate(piece_refs):
        offset = pl.multiple_of((tp_index ^ k) * cols, 128)
        mod_ref[:, pl.ds(offset, cols)] = piece[...]
    factor_ref[...] = gain_ref[...] * (1.0 + mod_ref[SCALE : SCALE + 1, :])
    offset_ref[...] = jnp.broadcast_to(mod_ref[SHIFT : SHIFT + 1, :], offset_ref.shape)
    step = 16

    def body(i, carry):
        at = pl.ds(pl.multiple_of(i * step, step), step)
        inverse = inverse_ref[at, :].reshape(step // 8, 8, 128)
        for j in range(0, model, 128):
            lanes = slice(j, j + 128)
            floats = latent_ref[at, lanes].astype(F32).reshape(step // 8, 8, 128)
            result = floats * inverse * factor_ref[:, lanes][None] + offset_ref[:, lanes][None]
            normed_ref[at, lanes] = result.reshape(step, 128).astype(BF16)
        return carry

    lax.fori_loop(0, tokens // step, body, 0, unroll=4)
    for kv_ref, weight_ref in zip(kv_refs, weight_refs):
        kv_ref[...] = jnp.dot(
            normed_ref[...], weight_ref[...], preferred_element_type=F32
        ).astype(BF16)
    odd = lax.axis_index("sp") % 2
    send_halo(kv_refs, send_refs[:evens], 1 - odd)
    send_halo(kv_refs, send_refs[evens:], odd)


def query_kernel(normed_ref, wq_ref, latent_ref, q_ref, resid_ref):
    cols = resid_ref.shape[1]
    query = jnp.dot(normed_ref[...], wq_ref[...], preferred_element_type=F32)
    q_ref[...] = (query * (LOG2_E * HEAD_DIM**-0.5)).astype(BF16)
    own = pl.ds(pl.multiple_of(lax.axis_index("tp") * cols, 128), cols)
    resid_ref[...] = latent_ref[:, own]


def context_kernel(*refs, masks, chunks):
    mod_ref, gain_ref = refs[:2]
    piece_refs = refs[2 : 2 + len(masks)]
    weight_refs = refs[2 + len(masks) : 2 + len(masks) + chunks]
    out_refs, whole_ref = refs[2 + len(masks) + chunks : -1], refs[-1]
    cols = piece_refs[0].shape[1]
    tp_index = lax.axis_index("tp")
    for mask, piece in zip(masks, piece_refs):
        whole_ref[:, pl.ds(pl.multiple_of((tp_index ^ mask) * cols, 128), cols)] = piece[...]
    floats = whole_ref[...].astype(F32)
    factor = gain_ref[0:1, :] * (1.0 + mod_ref[CTX_SCALE : CTX_SCALE + 1, :])
    shift = mod_ref[CTX_SHIFT : CTX_SHIFT + 1, :]
    normed = (floats * inverse_rms(floats) * factor + shift).astype(BF16)
    for weight, out in zip(weight_refs, out_refs):
        out[...] = jnp.dot(normed, weight[...], preferred_element_type=F32).astype(BF16)


def attention_kernel(
    q_ref,
    kv_ref,
    recv_a_ref,
    recv_b_ref,
    table_ref,
    ctx_ref,
    out_ref,
    pad_ref,
    score_ref,
    weight_ref,
    *,
    chunk,
    sp_count,
):
    tokens, width = out_ref.shape
    heads = width // HEAD_DIM
    rows = tokens // GRID_W
    halo = HALO * GRID_W
    groups, keys, _ = score_ref.shape
    group = rows // groups
    ctx_rows = ctx_ref.shape[0]
    span = keys - ctx_rows
    sp_index = lax.axis_index("sp")
    odd = sp_index % 2
    far = halo + tokens
    for recv_ref, side in ((recv_a_ref, 1 - odd), (recv_b_ref, odd)):
        lane = chunk * 2 * width if recv_ref.shape[1] > 2 * width else 0
        pad_ref[pl.ds(pl.multiple_of(side * far, GRID_W), halo), : 2 * width] = recv_ref[
            :, lane : lane + 2 * width
        ]
    pad_ref[halo : halo + tokens, : 2 * width] = kv_ref[...]
    lane_head = lax.broadcasted_iota(jnp.int32, (1, width), 1) // HEAD_DIM
    picks = [(lane_head == h) for h in range(heads)]
    nt = (((1,), (1,)), ((), ()))
    tn = (((0,), (0,)), ((), ()))

    def start_of(l):
        grid_row = sp_index * rows + l
        first = jnp.clip(grid_row - HALO, 0, sp_count * rows - WIN_H)
        return first - sp_index * rows + HALO, first - grid_row + WIN_H - 1

    def window_of(g):
        return pl.ds(pl.multiple_of(start_of(g * group)[0] * GRID_W, GRID_W), span)

    def score(g):
        left, bias = [], []
        first_start = start_of(g * group)[0]
        for k in range(group):
            l = g * group + k
            query = q_ref[l * GRID_W : (l + 1) * GRID_W, chunk * width : (chunk + 1) * width]
            left += [jnp.where(pick, query, BF16(0)) for pick in picks]
            start, offset = start_of(l)
            shift = start - first_start
            blocks = []
            for u in range(span // GRID_W):
                row = jnp.clip(u - shift, 0, WIN_H - 1) + offset
                block = table_ref[pl.ds(pl.multiple_of(row * GRID_W, GRID_W), GRID_W), :]
                if k == 0 and u >= WIN_H:
                    block = jnp.full_like(block, MASKED)
                elif u < k or u >= WIN_H:
                    block = jnp.where((u >= shift) & (u < shift + WIN_H), block, MASKED)
                blocks.append(block)
            bias.append(jnp.concatenate(blocks, axis=0))
        left = jnp.concatenate(left, axis=0)
        scores = jnp.concatenate(bias, axis=1) + lax.dot_general(
            pad_ref[window_of(g), :width], left, nt, preferred_element_type=F32
        )
        ctx_scores = lax.dot_general(ctx_ref[:, :width], left, nt, preferred_element_type=F32)
        score_ref[g, :span, :] = scores
        score_ref[g, span:, :] = ctx_scores
        return jnp.maximum(
            jnp.max(scores, axis=0, keepdims=True), jnp.max(ctx_scores, axis=0, keepdims=True)
        )

    def weigh(g, highest):
        partial = None
        for at in range(0, keys, 32):
            weights = jnp.exp2(score_ref[g, at : at + 32, :] - highest)
            weight_ref[g, at : at + 32, :] = weights.astype(BF16)
            folded = jnp.sum(weights.reshape(4, 8, -1), axis=0)
            partial = folded if partial is None else partial + folded
        return 1.0 / jnp.sum(partial, axis=0, keepdims=True)

    def mix(g, scale):
        mixed = lax.dot_general(
            pad_ref[window_of(g), width:], weight_ref[g, :span, :], tn, preferred_element_type=F32
        ) + lax.dot_general(
            ctx_ref[:, width:], weight_ref[g, span:, :], tn, preferred_element_type=F32
        )
        mixed = mixed * scale
        for k in range(group):
            turned = mixed[:, k * width : (k + 1) * width].T
            result = turned[:GRID_W]
            for h in range(1, heads):
                result = jnp.where(picks[h], turned[h * GRID_W : (h + 1) * GRID_W], result)
            l = g * group + k
            out_ref[l * GRID_W : (l + 1) * GRID_W, :] = result.astype(BF16)

    highest = [score(g) for g in range(groups)]
    scales = []
    for g in range(groups):
        scales.append(weigh(g, highest[g]))
        if g > 0:
            mix(g - 1, scales[g - 1])
    mix(groups - 1, scales[-1])


def output_kernel(*refs, masks, chunk, chunks):
    count = len(masks)
    w_out_ref, piece_refs = refs[0], refs[1 : 1 + count]
    more, out_ref = list(refs[1 + count : -1]), refs[-1]
    tp_index = lax.axis_index("tp")
    each = piece_refs[0].shape[1]
    rows = [
        w_out_ref[pl.ds(pl.multiple_of(((tp_index ^ m) * chunks + chunk) * each, 128), each), :]
        for m in masks
    ]
    branch = jnp.dot(
        jnp.concatenate([piece[...] for piece in piece_refs], axis=1),
        jnp.concatenate(rows, axis=0),
        preferred_element_type=F32,
    )
    if chunk > 0:
        branch = branch + more.pop(0)[...]
    if chunk == chunks - 1:
        resid_ref, mod_ref = more
        branch = resid_ref[...].astype(F32) + mod_ref[GATE : GATE + 1, :] * branch
    out_ref[...] = branch.astype(out_ref.dtype)


def local(
    latent,
    conditioning,
    context,
    ctx_vector,
    w_shift,
    w_scale,
    w_gate,
    norm_gain,
    w_query,
    w_key,
    w_value,
    offset_bias,
    w_out,
):
    tokens, model = latent.shape
    cols = w_shift.shape[1]
    width = w_query.shape[1]
    heads = width // HEAD_DIM
    chunks = width // 128 if width % 128 == 0 else 1
    each = width // chunks
    sp_count, tp_count = lax.axis_size("sp"), lax.axis_size("tp")
    halo = HALO * GRID_W

    own_context = shape_of((context.shape[0], cols), BF16)
    mod_inputs = (conditioning, ctx_vector, w_shift, w_scale, w_gate)
    partial = call(
        modulation_kernel,
        shape_of((2 * MOD_ROWS + context.shape[0], cols), BF16),
        scratch=[pltpu.VMEM(a.shape, a.dtype) for a in mod_inputs + (own_context,)]
        + [pltpu.SemaphoreType.DMA((6,))],
        in_specs=[HBM] * 6,
    )(*in_hbm(mod_inputs + (context,)))
    mod_own, ctx_own = total_and_context(partial, "sp")
    mod_pieces = pieces_of(mod_own, "tp")

    fill = GRID_W - offset_bias.shape[2]
    flipped = jnp.pad(offset_bias[:, :, ::-1], ((0, 0), (0, 0), (0, fill)))
    vectors = [
        jnp.concatenate(list(flipped[c * heads // chunks : (c + 1) * heads // chunks]), axis=1)
        for c in range(chunks)
    ]
    table_shape = shape_of(((2 * WIN_H - 1) * GRID_W, each), F32)
    inverse, gain, *prepared = call(
        functools.partial(prepare_kernel, chunks=chunks),
        (shape_of((tokens, 128), F32), shape_of((8, model), F32))
        + (shape_of((model, 2 * each), BF16),) * chunks
        + (table_shape,) * chunks,
        scratch=[pltpu.VMEM((model,), BF16), pltpu.SemaphoreType.DMA((1 + 2 * chunks,))],
        in_specs=[VMEM] + [HBM] * 3 + [VMEM] * chunks,
    )(latent, *in_hbm((norm_gain, w_key, w_value)), *vectors)
    weights, tables = prepared[:chunks], prepared[chunks:]

    evens, odds = 1, chunks
    normed, mod, *projected = call(
        functools.partial(norm_kernel, chunks=chunks, tp_count=tp_count, evens=evens),
        (shape_of((tokens, model), BF16), shape_of((MOD_ROWS, model), F32))
        + (shape_of((tokens, 2 * each), BF16),) * chunks
        + (shape_of((halo, 2 * width // evens), BF16),) * evens
        + (shape_of((halo, 2 * width // odds), BF16),) * odds,
        scratch=[pltpu.VMEM((8, model), F32), pltpu.VMEM((8, model), F32)],
    )(latent, inverse, gain, *weights, *mod_pieces)
    keys_values, sends = projected[:chunks], projected[chunks:]
    from_even = [pairwise(s, "sp", 0) for s in sends[:evens]]
    from_odd = [pairwise(s, "sp", 1) for s in sends[evens:]]

    query, resid = call(
        query_kernel, (shape_of((tokens, width), BF16), shape_of((tokens, cols), BF16))
    )(normed, w_query, latent)

    ctx_pieces = pieces_by_bits(ctx_own, "tp")
    ctx_rows = ctx_own.shape[0]
    ctx_call = call(
        functools.partial(context_kernel, masks=[m for m, _ in ctx_pieces], chunks=chunks),
        (shape_of((ctx_rows, 2 * each), BF16),) * chunks,
        scratch=[pltpu.VMEM((ctx_rows, model), BF16)],
    )
    ctx_all = ctx_call(mod, gain, *[p for _, p in ctx_pieces], *weights)

    rows = tokens // GRID_W
    group = 2 if rows % 2 == 0 else 1
    keys = (WIN_H + group - 1) * GRID_W + ctx_rows
    branch = []
    for c in range(chunks):
        attended = call(
            functools.partial(attention_kernel, chunk=c, sp_count=sp_count),
            shape_of((tokens, each), BF16),
            scratch=[
                pltpu.VMEM((tokens + 2 * halo, 2 * each), BF16),
                pltpu.VMEM((rows // group, keys, group * each), F32),
                pltpu.VMEM((rows // group, keys, group * each), BF16),
            ],
        )(
            query,
            keys_values[c],
            from_even[min(c, evens - 1)],
            from_odd[min(c, odds - 1)],
            tables[c],
            ctx_all[c],
        )
        found = pieces_by_bits(attended, "tp")
        last = c == chunks - 1
        branch = [
            call(
                functools.partial(
                    output_kernel, masks=[m for m, _ in found], chunk=c, chunks=chunks
                ),
                shape_of((tokens, cols), BF16 if last else F32),
            )(w_out, *[p for _, p in found], *branch, *([resid, mod_own] if last else []))
        ]
    return branch[0]


def solution(mesh):
    return jax.shard_map(
        local,
        mesh=mesh,
        in_specs=(
            P(("grp", "sp"), None),
            P(("grp", "sp")),
            P(("grp", "sp"), None),
            P("sp"),
            P("sp", "tp"),
            P("sp", "tp"),
            P("sp", "tp"),
            P(),
            P(None, "tp"),
            P(None, "tp"),
            P(None, "tp"),
            P("tp", None, None),
            P(None, "tp"),
        ),
        out_specs=P(("grp", "sp"), "tp"),
        check_vma=False,
    )
```

```python
import functools

import jax
import jax.numpy as jnp
from jax import lax
from jax.experimental import pallas as pl
from jax.experimental.pallas import tpu as pltpu
from jax.sharding import PartitionSpec as P


HEAD_DIM = 64
GRID_W = 64
WIN_H = 8
WIN_W = 16
EPSILON = 1e-06
HALO = WIN_H // 2
MASKED = -1e30
OUT_BLOCKS = 3
PARTS = 1
LOG2_E = 1.4426950408889634
SHIFT, CTX_SHIFT, SCALE, CTX_SCALE, GATE, MOD_ROWS = 0, 1, 2, 3, 4, 8

HBM = pl.BlockSpec(memory_space=pltpu.HBM)
VMEM = pl.BlockSpec(memory_space=pltpu.VMEM)
F32 = jnp.float32
BF16 = jnp.bfloat16


def call(kernel, out_shape, scratch=(), vmem_mib=24, **kwargs):
    return pl.pallas_call(
        kernel,
        out_shape=out_shape,
        scratch_shapes=list(scratch),
        compiler_params=pltpu.CompilerParams(vmem_limit_bytes=vmem_mib * 2**20),
        **kwargs,
    )


def in_hbm(arrays):
    return [pltpu.with_memory_space_constraint(a, pltpu.HBM) for a in arrays]


def shape_of(shape, dtype):
    return jax.ShapeDtypeStruct(shape, dtype)


def digits(count):
    unit, found = 1, []
    while unit < count:
        radix = 4 if count // unit % 4 == 0 else 2
        found.append((unit, radix))
        unit *= radix
    return found


def peer(block, axis, mask):
    count = lax.axis_size(axis)
    return lax.ppermute(block, axis, [(i, i ^ mask) for i in range(count)])


def joined(parts):
    sums = None
    for part in parts:
        rows = part[:MOD_ROWS].astype(F32) + part[MOD_ROWS : 2 * MOD_ROWS].astype(F32)
        sums = rows if sums is None else sums + rows
    return sums, jnp.concatenate([part[2 * MOD_ROWS :] for part in parts], axis=0)


def total_and_context(block, axis):
    steps = digits(lax.axis_size(axis))
    for i, (unit, radix) in enumerate(steps):
        far_first = [peer(block, axis, unit * k) for k in reversed(range(1, radix))]
        sums, context = joined([block] + far_first)
        if i + 1 < len(steps):
            high = lax.reduce_precision(sums, 8, 7)
            block = jnp.concatenate([high, sums - high], axis=0).astype(BF16)
            block = jnp.concatenate([block, context], axis=0)
    return sums, context


def pieces_of(block, axis):
    pieces = [block]
    for unit, radix in digits(lax.axis_size(axis)):
        pieces = pieces + [peer(p, axis, unit * k) for k in range(1, radix) for p in pieces]
    return pieces


def pieces_by_bits(block, axis):
    pieces = [(0, block)]
    bit = lax.axis_size(axis) // 2
    while bit:
        pieces = pieces + [(mask ^ bit, peer(p, axis, bit)) for mask, p in pieces]
        bit //= 2
    return pieces


def pairwise(block, axis, first):
    count = lax.axis_size(axis)
    pairs = []
    for low in range(first, count - 1, 2):
        pairs += [(low, low + 1), (low + 1, low)]
    return lax.ppermute(block, axis, pairs)


def silu(v):
    return v / (1.0 + jnp.exp(-v))


def fetch(pairs, sems):
    copies = [
        pltpu.make_async_copy(source, target, sems.at[i]) for i, (source, target) in enumerate(pairs)
    ]
    for copy in copies:
        copy.start()
    return copies


def in_parts(source, target):
    step = target.shape[0] // PARTS
    parts = [pl.ds(i * step, step) for i in range(PARTS)]
    return [(source.at[at, :], target.at[at, :]) for at in parts]


def modulation_kernel(
    cond_hbm, ctx_hbm, w_shift_hbm, w_scale_hbm, w_gate_hbm, context_hbm, out_ref, *scratch
):
    cond_ref, ctx_ref, w_shift_ref, w_scale_ref, w_gate_ref, context_ref, sems = scratch
    cols = w_shift_ref.shape[1]
    own = pl.ds(pl.multiple_of(lax.axis_index("tp") * cols, 128), cols)
    pairs = [(cond_hbm, cond_ref), (ctx_hbm, ctx_ref)]
    for source, target in (
        (w_shift_hbm, w_shift_ref),
        (w_scale_hbm, w_scale_ref),
        (w_gate_hbm, w_gate_ref),
    ):
        pairs += in_parts(source, target)
    copies = fetch(pairs + [(context_hbm.at[:, own], context_ref)], sems)
    copies[0].wait()
    copies[1].wait()

    def product(weight_ref, at):
        for copy in copies[2 + at * PARTS : 2 + (at + 1) * PARTS]:
            copy.wait()
        return jnp.dot(acts, weight_ref[...], preferred_element_type=F32)

    cond = silu(cond_ref[...].astype(F32)).reshape(1, -1)
    ctx = silu(ctx_ref[...].astype(F32)).reshape(1, -1)
    row = lax.broadcasted_iota(jnp.int32, (MOD_ROWS, cond.shape[1]), 0)
    acts = jnp.where(row % 2 == 0, cond, ctx).astype(BF16)
    shifts = product(w_shift_ref, 0)
    scales = product(w_scale_ref, 1)
    gates = product(w_gate_ref, 2)
    out_row = lax.broadcasted_iota(jnp.int32, shifts.shape, 0)
    sums = jnp.where(out_row < SCALE, shifts, jnp.where(out_row < GATE, scales, gates))
    high = sums.astype(BF16).astype(F32)
    out_ref[: 2 * MOD_ROWS, :] = jnp.concatenate([high, sums - high], axis=0).astype(BF16)
    copies[-1].wait()
    out_ref[2 * MOD_ROWS :, :] = context_ref[...]


def bias_table(vectors_ref, out_ref):
    lanes = out_ref.shape[1]
    key = lax.broadcasted_iota(jnp.int32, (GRID_W, lanes), 0)
    query = lax.broadcasted_iota(jnp.int32, (GRID_W, lanes), 1) % GRID_W
    first = jnp.clip(query - WIN_W // 2, 0, GRID_W - WIN_W)
    inside = (key >= first) & (key < first + WIN_W)
    for r in range(2 * WIN_H - 1):
        table = pltpu.roll(
            jnp.broadcast_to(vectors_ref[r : r + 1, :], (GRID_W, lanes)),
            lanes - (WIN_W - 1),
            1,
            stride=1,
            stride_axis=0,
        )
        out_ref[r * GRID_W : (r + 1) * GRID_W, :] = jnp.where(inside, table * LOG2_E, MASKED)


def inverse_rms(floats):
    return lax.rsqrt(jnp.mean(floats * floats, axis=-1, keepdims=True) + EPSILON)


def send_halo(kv_refs, send_refs, low_side):
    halo, _ = send_refs[0].shape
    at = pl.ds(pl.multiple_of(low_side * (kv_refs[0].shape[0] - halo), GRID_W), halo)
    each = kv_refs[0].shape[1]
    for c, kv_ref in enumerate(kv_refs):
        if len(send_refs) > 1:
            send_refs[c][...] = kv_ref[at, :]
        else:
            send_refs[0][:, c * each : (c + 1) * each] = kv_ref[at, :]


def prepare_kernel(*refs, chunks):
    latent_ref, gain_hbm, wk_hbm, wv_hbm = refs[:4]
    vector_refs = refs[4 : 4 + chunks]
    inverse_ref, gain_out_ref = refs[4 + chunks : 6 + chunks]
    weight_refs = refs[6 + chunks : 6 + 2 * chunks]
    table_refs = refs[6 + 2 * chunks : -2]
    gain_ref, sems = refs[-2:]
    tokens, _ = latent_ref.shape
    each = weight_refs[0].shape[1] // 2
    pairs = [(gain_hbm, gain_ref)]
    for c, weight in enumerate(weight_refs):
        at = pl.ds(c * each, each)
        pairs += [(wk_hbm.at[:, at], weight.at[:, :each]), (wv_hbm.at[:, at], weight.at[:, each:])]
    copies = fetch(pairs, sems)
    for vectors_ref, table_ref in zip(vector_refs, table_refs):
        bias_table(vectors_ref, table_ref)
    step = 16

    def body(i, carry):
        at = pl.ds(pl.multiple_of(i * step, step), step)
        inverse = inverse_rms(latent_ref[at, :].astype(F32))
        inverse_ref[at, :] = jnp.broadcast_to(inverse, (step, 128))
        return carry

    lax.fori_loop(0, tokens // step, body, 0, unroll=2)
    copies[0].wait()
    gain = gain_ref[...].astype(F32).reshape(1, -1)
    gain_out_ref[...] = jnp.broadcast_to(gain, gain_out_ref.shape)
    for copy in copies[1:]:
        copy.wait()


def norm_kernel(*refs, chunks, tp_count, evens):
    latent_ref, inverse_ref, gain_ref = refs[:3]
    weight_refs, piece_refs = refs[3 : 3 + chunks], refs[3 + chunks : 3 + chunks + tp_count]
    normed_ref, mod_ref = refs[3 + chunks + tp_count : 5 + chunks + tp_count]
    kv_refs = refs[5 + chunks + tp_count : 5 + 2 * chunks + tp_count]
    send_refs = refs[5 + 2 * chunks + tp_count : -2]
    factor_ref, offset_ref = refs[-2:]
    tokens, model = latent_ref.shape
    cols = piece_refs[0].shape[1]
    tp_index = lax.axis_index("tp")
    for k, piece in enumerate(piece_refs):
        offset = pl.multiple_of((tp_index ^ k) * cols, 128)
        mod_ref[:, pl.ds(offset, cols)] = piece[...]
    factor_ref[...] = gain_ref[...] * (1.0 + mod_ref[SCALE : SCALE + 1, :])
    offset_ref[...] = jnp.broadcast_to(mod_ref[SHIFT : SHIFT + 1, :], offset_ref.shape)
    step = 16

    def body(i, carry):
        at = pl.ds(pl.multiple_of(i * step, step), step)
        inverse = inverse_ref[at, :].reshape(step // 8, 8, 128)
        for j in range(0, model, 128):
            lanes = slice(j, j + 128)
            floats = latent_ref[at, lanes].astype(F32).reshape(step // 8, 8, 128)
            result = floats * inverse * factor_ref[:, lanes][None] + offset_ref[:, lanes][None]
            normed_ref[at, lanes] = result.reshape(step, 128).astype(BF16)
        return carry

    lax.fori_loop(0, tokens // step, body, 0, unroll=4)
    for kv_ref, weight_ref in zip(kv_refs, weight_refs):
        kv_ref[...] = jnp.dot(
            normed_ref[...], weight_ref[...], preferred_element_type=F32
        ).astype(BF16)
    odd = lax.axis_index("sp") % 2
    send_halo(kv_refs, send_refs[:evens], 1 - odd)
    send_halo(kv_refs, send_refs[evens:], odd)


def query_kernel(normed_ref, wq_ref, latent_ref, q_ref, resid_ref):
    cols = resid_ref.shape[1]
    query = jnp.dot(normed_ref[...], wq_ref[...], preferred_element_type=F32)
    q_ref[...] = (query * (LOG2_E * HEAD_DIM**-0.5)).astype(BF16)
    own = pl.ds(pl.multiple_of(lax.axis_index("tp") * cols, 128), cols)
    resid_ref[...] = latent_ref[:, own]


def context_kernel(*refs, masks, chunks):
    mod_ref, gain_ref = refs[:2]
    piece_refs = refs[2 : 2 + len(masks)]
    weight_refs = refs[2 + len(masks) : 2 + len(masks) + chunks]
    out_refs, whole_ref = refs[2 + len(masks) + chunks : -1], refs[-1]
    cols = piece_refs[0].shape[1]
    tp_index = lax.axis_index("tp")
    for mask, piece in zip(masks, piece_refs):
        whole_ref[:, pl.ds(pl.multiple_of((tp_index ^ mask) * cols, 128), cols)] = piece[...]
    floats = whole_ref[...].astype(F32)
    factor = gain_ref[0:1, :] * (1.0 + mod_ref[CTX_SCALE : CTX_SCALE + 1, :])
    shift = mod_ref[CTX_SHIFT : CTX_SHIFT + 1, :]
    normed = (floats * inverse_rms(floats) * factor + shift).astype(BF16)
    for weight, out in zip(weight_refs, out_refs):
        out[...] = jnp.dot(normed, weight[...], preferred_element_type=F32).astype(BF16)


def attention_kernel(
    q_ref,
    kv_ref,
    recv_a_ref,
    recv_b_ref,
    table_ref,
    ctx_ref,
    out_ref,
    pad_ref,
    score_ref,
    weight_ref,
    *,
    chunk,
    sp_count,
):
    tokens, width = out_ref.shape
    heads = width // HEAD_DIM
    rows = tokens // GRID_W
    halo = HALO * GRID_W
    groups, keys, _ = score_ref.shape
    group = rows // groups
    ctx_rows = ctx_ref.shape[0]
    span = keys - ctx_rows
    sp_index = lax.axis_index("sp")
    odd = sp_index % 2
    far = halo + tokens
    for recv_ref, side in ((recv_a_ref, 1 - odd), (recv_b_ref, odd)):
        lane = chunk * 2 * width if recv_ref.shape[1] > 2 * width else 0
        pad_ref[pl.ds(pl.multiple_of(side * far, GRID_W), halo), : 2 * width] = recv_ref[
            :, lane : lane + 2 * width
        ]
    pad_ref[halo : halo + tokens, : 2 * width] = kv_ref[...]
    lane_head = lax.broadcasted_iota(jnp.int32, (1, width), 1) // HEAD_DIM
    picks = [(lane_head == h) for h in range(heads)]
    nt = (((1,), (1,)), ((), ()))
    tn = (((0,), (0,)), ((), ()))

    def start_of(l):
        grid_row = sp_index * rows + l
        first = jnp.clip(grid_row - HALO, 0, sp_count * rows - WIN_H)
        return first - sp_index * rows + HALO, first - grid_row + WIN_H - 1

    def window_of(g):
        return pl.ds(pl.multiple_of(start_of(g * group)[0] * GRID_W, GRID_W), span)

    def score(g):
        left, bias = [], []
        first_start = start_of(g * group)[0]
        for k in range(group):
            l = g * group + k
            query = q_ref[l * GRID_W : (l + 1) * GRID_W, chunk * width : (chunk + 1) * width]
            left += [jnp.where(pick, query, BF16(0)) for pick in picks]
            start, offset = start_of(l)
            shift = start - first_start
            blocks = []
            for u in range(span // GRID_W):
                row = jnp.clip(u - shift, 0, WIN_H - 1) + offset
                block = table_ref[pl.ds(pl.multiple_of(row * GRID_W, GRID_W), GRID_W), :]
                if k == 0 and u >= WIN_H:
                    block = jnp.full_like(block, MASKED)
                elif u < k or u >= WIN_H:
                    block = jnp.where((u >= shift) & (u < shift + WIN_H), block, MASKED)
                blocks.append(block)
            bias.append(jnp.concatenate(blocks, axis=0))
        left = jnp.concatenate(left, axis=0)
        scores = jnp.concatenate(bias, axis=1) + lax.dot_general(
            pad_ref[window_of(g), :width], left, nt, preferred_element_type=F32
        )
        ctx_scores = lax.dot_general(ctx_ref[:, :width], left, nt, preferred_element_type=F32)
        score_ref[g, :span, :] = scores
        score_ref[g, span:, :] = ctx_scores
        return jnp.maximum(
            jnp.max(scores, axis=0, keepdims=True), jnp.max(ctx_scores, axis=0, keepdims=True)
        )

    def weigh(g, highest):
        partial = None
        for at in range(0, keys, 32):
            weights = jnp.exp2(score_ref[g, at : at + 32, :] - highest)
            weight_ref[g, at : at + 32, :] = weights.astype(BF16)
            folded = jnp.sum(weights.reshape(4, 8, -1), axis=0)
            partial = folded if partial is None else partial + folded
        return 1.0 / jnp.sum(partial, axis=0, keepdims=True)

    def mix(g, scale):
        mixed = lax.dot_general(
            pad_ref[window_of(g), width:], weight_ref[g, :span, :], tn, preferred_element_type=F32
        ) + lax.dot_general(
            ctx_ref[:, width:], weight_ref[g, span:, :], tn, preferred_element_type=F32
        )
        mixed = mixed * scale
        for k in range(group):
            turned = mixed[:, k * width : (k + 1) * width].T
            result = turned[:GRID_W]
            for h in range(1, heads):
                result = jnp.where(picks[h], turned[h * GRID_W : (h + 1) * GRID_W], result)
            l = g * group + k
            out_ref[l * GRID_W : (l + 1) * GRID_W, :] = result.astype(BF16)

    highest = [score(g) for g in range(groups)]
    scales = []
    for g in range(groups):
        scales.append(weigh(g, highest[g]))
        if g > 0:
            mix(g - 1, scales[g - 1])
    mix(groups - 1, scales[-1])


def output_kernel(*refs, places, blocks):
    w_out_ref, mod_ref, before_ref = refs[:3]
    piece_refs, more = refs[3 : 3 + len(places)], refs[3 + len(places) :]
    tp_index = lax.axis_index("tp")
    each = piece_refs[0].shape[1]
    rows = [
        w_out_ref[pl.ds(pl.multiple_of(((tp_index ^ mask) * of + chunk) * each, 128), each), :]
        for mask, chunk, of in places
    ]
    weight = jnp.concatenate(rows, axis=0)
    gate = mod_ref[GATE : GATE + 1, :]

    def updated(at):
        pieces = jnp.concatenate([piece[at, :] for piece in piece_refs], axis=1)
        product = jnp.dot(pieces, weight, preferred_element_type=F32)
        return before_ref[at, :].astype(F32) + gate * product

    if not blocks:
        more[0][...] = updated(slice(None))
        return
    out_hbm, out_ref, sems = more
    step = out_ref.shape[0] // blocks
    copies = []
    for i in range(blocks):
        at = pl.ds(i * step, step)
        out_ref[at, :] = updated(at).astype(BF16)
        copies += fetch([(out_ref.at[at, :], out_hbm.at[at, :])], sems.at[pl.ds(i, 1)])
    for copy in copies:
        copy.wait()


def local(
    latent,
    conditioning,
    context,
    ctx_vector,
    w_shift,
    w_scale,
    w_gate,
    norm_gain,
    w_query,
    w_key,
    w_value,
    offset_bias,
    w_out,
):
    tokens, model = latent.shape
    cols = w_shift.shape[1]
    width = w_query.shape[1]
    heads = width // HEAD_DIM
    chunks = width // 128 if width % 128 == 0 else 1
    each = width // chunks
    sp_count, tp_count = lax.axis_size("sp"), lax.axis_size("tp")
    halo = HALO * GRID_W

    own_context = shape_of((context.shape[0], cols), BF16)
    mod_inputs = (conditioning, ctx_vector, w_shift, w_scale, w_gate)
    partial = call(
        modulation_kernel,
        shape_of((2 * MOD_ROWS + context.shape[0], cols), BF16),
        scratch=[pltpu.VMEM(a.shape, a.dtype) for a in mod_inputs + (own_context,)]
        + [pltpu.SemaphoreType.DMA((3 + 3 * PARTS,))],
        in_specs=[HBM] * 6,
    )(*in_hbm(mod_inputs + (context,)))
    mod_own, ctx_own = total_and_context(partial, "sp")
    mod_pieces = pieces_of(mod_own, "tp")

    fill = GRID_W - offset_bias.shape[2]
    flipped = jnp.pad(offset_bias[:, :, ::-1], ((0, 0), (0, 0), (0, fill)))
    vectors = [
        jnp.concatenate(list(flipped[c * heads // chunks : (c + 1) * heads // chunks]), axis=1)
        for c in range(chunks)
    ]
    table_shape = shape_of(((2 * WIN_H - 1) * GRID_W, each), F32)
    inverse, gain, *prepared = call(
        functools.partial(prepare_kernel, chunks=chunks),
        (shape_of((tokens, 128), F32), shape_of((8, model), F32))
        + (shape_of((model, 2 * each), BF16),) * chunks
        + (table_shape,) * chunks,
        scratch=[pltpu.VMEM((model,), BF16), pltpu.SemaphoreType.DMA((1 + 2 * chunks,))],
        in_specs=[VMEM] + [HBM] * 3 + [VMEM] * chunks,
    )(latent, *in_hbm((norm_gain, w_key, w_value)), *vectors)
    weights, tables = prepared[:chunks], prepared[chunks:]

    evens, odds = 1, chunks
    normed, mod, *projected = call(
        functools.partial(norm_kernel, chunks=chunks, tp_count=tp_count, evens=evens),
        (shape_of((tokens, model), BF16), shape_of((MOD_ROWS, model), F32))
        + (shape_of((tokens, 2 * each), BF16),) * chunks
        + (shape_of((halo, 2 * width // evens), BF16),) * evens
        + (shape_of((halo, 2 * width // odds), BF16),) * odds,
        scratch=[pltpu.VMEM((8, model), F32), pltpu.VMEM((8, model), F32)],
    )(latent, inverse, gain, *weights, *mod_pieces)
    keys_values, sends = projected[:chunks], projected[chunks:]
    from_even = [pairwise(s, "sp", 0) for s in sends[:evens]]
    from_odd = [pairwise(s, "sp", 1) for s in sends[evens:]]

    query, resid = call(
        query_kernel, (shape_of((tokens, width), BF16), shape_of((tokens, cols), BF16))
    )(normed, w_query, latent)

    ctx_pieces = pieces_by_bits(ctx_own, "tp")
    ctx_rows = ctx_own.shape[0]
    ctx_call = call(
        functools.partial(context_kernel, masks=[m for m, _ in ctx_pieces], chunks=chunks),
        (shape_of((ctx_rows, 2 * each), BF16),) * chunks,
        scratch=[pltpu.VMEM((ctx_rows, model), BF16)],
    )
    ctx_all = ctx_call(mod, gain, *[p for _, p in ctx_pieces], *weights)

    rows = tokens // GRID_W
    group = 2 if rows % 2 == 0 else 1
    keys = (WIN_H + group - 1) * GRID_W + ctx_rows
    arrived = []
    for c in range(chunks):
        attended = call(
            functools.partial(attention_kernel, chunk=c, sp_count=sp_count),
            shape_of((tokens, each), BF16),
            scratch=[
                pltpu.VMEM((tokens + 2 * halo, 2 * each), BF16),
                pltpu.VMEM((rows // group, keys, group * each), F32),
                pltpu.VMEM((rows // group, keys, group * each), BF16),
            ],
        )(
            query,
            keys_values[c],
            from_even[min(c, evens - 1)],
            from_odd[min(c, odds - 1)],
            tables[c],
            ctx_all[c],
        )
        found = pieces_by_bits(attended, "tp")
        arrived += [((mask, c, chunks), piece) for mask, piece in found]

    stages = [[], [], []]
    for place, piece in arrived:
        late = place[1] == chunks - 1 and place[0] > 1
        stages[1 + place[0] % 2 if late else 0].append((place, piece))
    stages = [stage for stage in stages if stage]
    result = resid
    for s, stage in enumerate(stages):
        last = s == len(stages) - 1
        result = call(
            functools.partial(
                output_kernel,
                places=[place for place, _ in stage],
                blocks=OUT_BLOCKS if last else 0,
            ),
            shape_of((tokens, cols), BF16 if last else F32),
            scratch=[
                pltpu.VMEM((tokens, cols), BF16),
                pltpu.SemaphoreType.DMA((OUT_BLOCKS,)),
            ]
            if last
            else [],
            **(dict(out_specs=HBM) if last else {}),
        )(w_out, mod_own, result, *[piece for _, piece in stage])
    return result


def solution(mesh):
    return jax.shard_map(
        local,
        mesh=mesh,
        in_specs=(
            P(("grp", "sp"), None),
            P(("grp", "sp")),
            P(("grp", "sp"), None),
            P("sp"),
            P("sp", "tp"),
            P("sp", "tp"),
            P("sp", "tp"),
            P(),
            P(None, "tp"),
            P(None, "tp"),
            P(None, "tp"),
            P("tp", None, None),
            P(None, "tp"),
        ),
        out_specs=P(("grp", "sp"), "tp"),
        check_vma=False,
    )
```
